256 devices in a mesh: grp: 2 (over z), ep: 64 (over y, x), tp: 2 (over core).
Axes of the slice: x: 8, y: 8, z: 2, core: 2. Of those that a mesh axis runs over, the one named last changes fastest.
The devices are a block of a 8x8x16 slice.
Arguments:
- tokens: bfloat16 [65536, 2048], P(('grp', 'ep'), 'tp'), parts along dimension 0, may hold values from -6 to 6
- norm_gain: float32 [2048], replicated, may hold values from 0.1 to 1.9
- expert_ids: int32 [65536, 2], P(('grp', 'ep')), parts along dimension 0, may hold values from 0 to 63, all different within a row; in each aligned block of 512 rows (0 to 511, 512 to 1023, ...) at most 24 rows name the same one
- route_weights: float32 [65536, 2], P(('grp', 'ep')), parts along dimension 0, may hold values from 0.1 to 1
- gate_weight: bfloat16 [64, 2048, 512], P('ep', None, 'tp'), may hold values from -0.125 to 0.125
- up_weight: bfloat16 [64, 2048, 512], P('ep', None, 'tp'), may hold values from -0.125 to 0.125
- down_weight: bfloat16 [64, 512, 2048], P('ep', None, 'tp'), may hold values from -0.25 to 0.25
Outputs:
- mixed: bfloat16 [65536, 2048], P(('grp', 'ep'), 'tp'), parts along dimension 0
The draws below stay inside these ranges and needn't reach their ends.
There are 2 independent parts, one for each index of `grp`. The reference program is written for one: setup_inputs(seed, part) draws one part's arguments, and reference() takes and returns one part's arrays. A program takes and returns all parts, laid end to end along the dimension named above; an argument that names none is the same for every part. Nothing has to cross between parts.
Inputs may be any that keep to these rules, and one draw needn't show every extreme that they name: `expert_ids`: each token names 2 different experts. Among the 512 tokens of one index of ep (aligned blocks of rows) at most 24 name the same expert, and in some block some expert is named by exactly 24 of them.
All inputs are finite; a program needn't handle non-finite values.
Results may differ from the reference program's by a relative error of at most 0.007.
Values may be sent and summed in bfloat16 or wider, within the bound.
A program may use at most 64 MiB of HBM per device.

```python
import math
import jax
import jax.numpy as jnp
import numpy as np
from jax import lax

D = 2048
DE = 512
TOP_K = 2
TOK_DEV = 512
EXPERTS = 64
TOKENS = 32768
CAP = 24
N_EP = 64


def levels(key, dims, pieces, least, high):
    def one(dim, parts):
        draws = jax.random.uniform(jax.random.fold_in(jax.random.fold_in(key, 6), dim), (parts,), jnp.float32, least / len(pieces), high / len(pieces))
        return jnp.repeat(jnp.exp(draws), dims[dim] // parts).reshape((-1,) + (1,) * (len(dims) - dim - 1))

    factor_of = one(*pieces[0])
    for cut in pieces[1:]:
        factor_of = factor_of * one(*cut)
    return factor_of


def shared_out(own_key, own, number, rows, amount, top, bound, lean):
    sequence = jax.random.permutation(own_key, amount)
    crowded, ordinary = shares(amount, rows * top, bound, lean, True), shares(amount, rows * top, bound, lean, False)
    places = jnp.arange(amount)

    def named(lengths, turn):
        used = int((lengths > 0).sum())
        fixed = max(1, used // 4)
        passed = fixed + (places - fixed + turn * (used - fixed)) % max(1, amount - fixed)
        return jnp.zeros((amount,), jnp.int32).at[sequence[jnp.where(places < fixed, places, passed)]].set(jnp.asarray(lengths, jnp.int32))

    lengths = jnp.where(number % 4 == 0, named(crowded, number // 4), named(ordinary, number - number // 4 - 1))
    mixed = jax.random.permutation(jax.random.fold_in(own, 3), amount)
    giver, receiver = mixed[0:amount // 2 * 2:2], mixed[1:amount // 2 * 2:2]
    room = jnp.minimum(lengths[giver] - 1, bound - lengths[receiver]) // 2
    room = jnp.where((giver == sequence[0]) | (receiver == sequence[0]) | (lengths[receiver] == 0), 0, jnp.maximum(room, 0))
    passed = jax.random.randint(jax.random.fold_in(own, 4), (amount // 2,), 0, 1 << 20) % (room + 1)
    lengths = lengths.at[giver].add(-passed).at[receiver].add(passed)
    labels = jnp.searchsorted(jnp.cumsum(lengths), jnp.arange(rows * top), side="right").astype(jnp.int32)
    table = labels.reshape(top, rows).T
    table = table[jax.random.permutation(jax.random.fold_in(own, 1), rows)]
    turn = jax.random.randint(jax.random.fold_in(own, 2), (rows, 1), 0, top)
    return jnp.take_along_axis(table, (jnp.arange(top)[None, :] + turn) % top, axis=1)


def shares(amount, total, bound, lean, full):
    portions = [(1 << 20) // math.isqrt(grade ** lean) + 1 for grade in range(1, amount + 1)]
    largest = bound if full else min(bound, max(-(-total // amount), total * portions[0] // sum(portions)))
    least = 1 if total - largest >= amount - 1 else 0
    counts, surplus = [largest] + [least] * (amount - 1), total - largest - least * (amount - 1)
    while surplus > 0:
        free = [i for i in range(1, amount) if counts[i] < largest] or [i for i in range(1, amount) if counts[i] < bound]
        whole, remaining = sum([portions[i] for i in free]), surplus
        for i in free:
            extra = min(bound - counts[i], max(1, remaining * portions[i] // whole), surplus)
            counts[i] = counts[i] + extra
            surplus = surplus - extra
    return np.array(counts)


def gaussian(own_key, extent, scale, limit, split=(), kind=jnp.bfloat16):
    entries = scale * jax.random.normal(own_key, extent, jnp.float32)
    if split:
        entries = entries * levels(own_key, extent, split, -0.22, 0.18)
    return jnp.clip(entries, -limit, limit).astype(kind)


def setup_inputs(seed: int = 0, part: int = 0) -> dict:
    key_of = jax.random.split(jax.random.key(seed), 8)
    own_keys = jax.random.split(jax.random.fold_in(key_of[7], part), 8)
    tokens = gaussian(own_keys[0], (TOKENS, D), 1.0, 6.0, ((0, 64), (1, 2)))
    norm_gain = jnp.clip(1.0 + 0.18 * jax.random.normal(key_of[1], (D,), jnp.float32), 0.1, 1.9)
    expert_ids_keys = jax.random.split(jax.random.fold_in(own_keys[2], 1), TOKENS // TOK_DEV)
    expert_ids_turns = jax.random.permutation(jax.random.fold_in(own_keys[2], 3), TOKENS // TOK_DEV)
    expert_ids = jax.vmap(lambda own, number: shared_out(jax.random.fold_in(own_keys[2], 2), own, number, TOK_DEV, EXPERTS, TOP_K, CAP, 2))(expert_ids_keys, expert_ids_turns).reshape((TOKENS, TOP_K))
    route_weights = jnp.clip(jnp.exp(math.log(1.0) - 2.3025851 * jax.random.uniform(own_keys[3], (TOKENS, TOP_K), jnp.float32) ** levels(own_keys[3], (TOKENS, TOP_K), ((0, 64),), -0.2, 0.2)), 0.1, 1.0)
    gate_weight = gaussian(key_of[4], (EXPERTS, D, DE), D ** -0.5, 0.125, ((0, 64), (2, 2)))
    up_weight = gaussian(key_of[5], (EXPERTS, D, DE), D ** -0.5, 0.125, ((0, 64), (2, 2)))
    down_weight = gaussian(key_of[6], (EXPERTS, DE, D), DE ** -0.5, 0.25, ((0, 64), (2, 2)))
    return dict(tokens=tokens, norm_gain=norm_gain, expert_ids=expert_ids, route_weights=route_weights, gate_weight=gate_weight, up_weight=up_weight, down_weight=down_weight)


def reference(tokens, norm_gain, expert_ids, route_weights, gate_weight, up_weight, down_weight):
    xf = tokens.astype(jnp.float32)
    scale = lax.rsqrt(lax.optimization_barrier(jnp.mean(xf * xf, axis=-1, keepdims=True)) + 1e-06)
    normed = (xf * scale * norm_gain.astype(jnp.float32)[None, :]).astype(jnp.bfloat16)
    flat = expert_ids.reshape(-1).astype(jnp.int32)
    pairs = flat.shape[0]
    onehot = (flat[:, None] == jnp.arange(EXPERTS, dtype=jnp.int32)[None, :]).astype(jnp.int32)
    blocked = onehot.reshape(-1, TOK_DEV * TOP_K, EXPERTS)
    earlier = (jnp.cumsum(blocked, axis=1) - blocked).reshape(pairs, EXPERTS)
    slot = lax.optimization_barrier(jnp.sum(earlier * onehot, axis=-1)).astype(jnp.int32)
    block = (jnp.arange(pairs, dtype=jnp.int32) // (TOK_DEV * TOP_K)).astype(jnp.int32)
    position = (block * CAP + slot).astype(jnp.int32)
    owner = (jnp.arange(pairs, dtype=jnp.int32) // TOP_K).astype(jnp.int32)
    source = jnp.full((EXPERTS, N_EP * CAP), TOKENS, jnp.int32).at[flat, position].set(owner)
    weights = jnp.zeros((EXPERTS, N_EP * CAP), jnp.float32).at[flat, position].set(route_weights.reshape(-1).astype(jnp.float32))
    padded = jnp.concatenate([normed, jnp.zeros((1, normed.shape[1]), jnp.bfloat16)], axis=0)

    def one_expert(total, inputs):
        rows_idx, row_w, w_gate, w_up, w_down = inputs
        rows = padded[rows_idx]
        gate = jnp.dot(rows, w_gate, preferred_element_type=jnp.float32)
        upper = jnp.dot(rows, w_up, preferred_element_type=jnp.float32)
        hidden = (jax.nn.silu(gate) * upper).astype(jnp.bfloat16)
        result = jnp.dot(hidden, w_down, preferred_element_type=jnp.float32).astype(jnp.bfloat16)
        total = total.at[rows_idx].add(result.astype(jnp.float32) * row_w[:, None])
        return (total, None)
    start = jnp.zeros((TOKENS + 1, normed.shape[1]), jnp.float32)
    total, _ = lax.scan(one_expert, start, (source, weights, gate_weight, up_weight, down_weight))
    return total[:TOKENS].astype(jnp.bfloat16)
```

```python
import functools
import math

import jax
import jax.numpy as jnp
from jax import lax
from jax.experimental import pallas as pl
from jax.experimental.pallas import tpu as pltpu
from jax.sharding import PartitionSpec as P

MESH = pl.DeviceIdType.MESH
BF16 = jnp.bfloat16
F32 = jnp.float32


def wrapped(v, side):
    v = jnp.where(v < 0, v + side, v)
    return jnp.where(v >= side, v - side, v)


def kernel(
    side, cap,
    tok, gain, ids, wts, gate_hbm, up_hbm, down_hbm, out,
    wg, wu, wd, snd, rl1, rcv, res, rl2, back, normed, acc, posr, wts_hi_lo,
    s_w, r_w, l_w, s_a, s_b, s_c, s_d, r1, r2, r3, r4,
):
    S = side
    c = lax.axis_index("tp")
    ep = lax.axis_index("ep")
    y = ep // S
    x = ep % S
    s = 1 - 2 * c
    tok_rows = tok.shape[0]
    half = tok.shape[1]
    blocks = cap // 8

    def at(dx, dy):
        return ((y + dy + S) % S) * S + (x + dx + S) % S

    def send(src, dst, send_sem, recv_sem, chip, core):
        pltpu.make_async_remote_copy(
            src_ref=src, dst_ref=dst, send_sem=send_sem, recv_sem=recv_sem,
            device_id={"ep": chip, "tp": core}, device_id_type=MESH,
        ).start()

    def wait(sem, ref):
        pltpu.make_async_copy(ref, ref, sem).wait()

    barrier = pltpu.get_barrier_semaphore()
    for d in range(1, S):
        for h in range(2):
            pl.semaphore_signal(barrier, inc=1, device_id={"ep": at(d, 0), "tp": h}, device_id_type=MESH)
            pl.semaphore_signal(barrier, inc=1, device_id={"ep": at(0, d), "tp": h}, device_id_type=MESH)
    pl.semaphore_signal(barrier, inc=1, device_id={"ep": ep, "tp": 1 - c}, device_id_type=MESH)

    weights = ((gate_hbm, wg), (up_hbm, wu), (down_hbm, wd))
    for i, (src, dst) in enumerate(weights):
        pltpu.make_async_copy(src.at[0], dst.at[c], l_w.at[i]).start()

    row = lax.broadcasted_iota(jnp.int32, (128, tok_rows), 0)
    e0 = ids[0:1, :]
    e1 = ids[1:2, :]
    hot0 = (row == e0).astype(F32)
    hot1 = (row == e1).astype(F32)
    earlier = (
        lax.broadcasted_iota(jnp.int32, (tok_rows, tok_rows), 0)
        < lax.broadcasted_iota(jnp.int32, (tok_rows, tok_rows), 1)
    )
    rank = jnp.dot(
        (hot0 + hot1).astype(BF16), earlier.astype(F32).astype(BF16), preferred_element_type=F32
    )
    pos0 = jnp.sum(rank * hot0, axis=0, keepdims=True) + (e0 * cap).astype(F32)
    pos1 = jnp.sum(rank * hot1, axis=0, keepdims=True) + (e1 * cap).astype(F32)
    w0 = wts[0:1, :]
    w1 = wts[1:2, :]
    w0_hi = w0.astype(BF16).astype(F32)
    w1_hi = w1.astype(BF16).astype(F32)
    row = lax.broadcasted_iota(jnp.int32, (8, tok_rows), 0)
    table = jnp.zeros((8, tok_rows), F32)
    for i, values in enumerate((pos0, pos1, w0_hi, w1_hi, w0 - w0_hi, w1 - w1_hi)):
        table = jnp.where(row == i, values, table)
    posr[...] = table
    table = jnp.concatenate([table, jnp.zeros((120, tok_rows), F32)], axis=0)
    wts_hi_lo[...] = jnp.transpose(table)

    def coords(j, k):
        t = (j + s * k + S) % S
        return t, j * (1 - c) + t * c, j * c + t * (1 - c)

    def positions(k, shape, dim):
        i = lax.broadcasted_iota(jnp.int32, shape, dim)
        j = jnp.zeros(shape, jnp.int32)
        for m in range(1, S):
            j = j + (i >= m * cap).astype(jnp.int32)
        t = wrapped(j + s * k, S)
        dx = jnp.where(c == 0, j, t)
        dy = jnp.where(c == 0, t, j)
        e = wrapped(y + dy, S) * S + wrapped(x + dx, S)
        return (e * cap + i - j * cap).astype(F32)

    def gather(k):
        p = positions(k, (S * cap, 1), 0)
        pick = jnp.where(p == posr[0:1, :], 1.0, jnp.where(p == posr[1:2, :], 1.0, 0.0))
        rows = jnp.dot(pick.astype(BF16), tok[...], preferred_element_type=F32)
        snd[k] = rows.reshape(S, blocks, 8, half).astype(BF16)

    def dispatch(k):
        for j in range(S):
            t, dx, dy = coords(j, k)
            p = dx % 2
            q = dx // 2
            if j == 0:
                @pl.when(t != 0)
                def _():
                    send(snd.at[k, j], rcv.at[k, q, c], s_a.at[k, j], r2.at[k, q, c], at(dx, dy), p)

                @pl.when((t == 0) & (c == 1))
                def _():
                    send(snd.at[k, j], rcv.at[k, q, c], s_a.at[k, j], r2.at[k, q, c], ep, 0)

                @pl.when((t == 0) & (c == 0))
                def _():
                    rcv[0, 0, 0] = snd[0, 0]
            else:
                @pl.when(t != 0)
                def _():
                    send(snd.at[k, j], rl1.at[k, j], s_a.at[k, j], r1.at[k, j], at(j * (1 - c), j * c), c)

                @pl.when(t == 0)
                def _():
                    send(snd.at[k, j], rcv.at[k, q, c], s_a.at[k, j], r2.at[k, q, c], at(dx, dy), p)

    def relay_dispatch(k):
        for j in range(1, S):
            t, dx, dy = coords(j, k)
            p = dx % 2
            q = dx // 2

            @pl.when(t != 0)
            def _():
                wait(r1.at[k, j], rl1.at[k, j])
                send(rl1.at[k, j], rcv.at[k, q, c], s_b.at[k, j], r2.at[k, q, c], at(t * c, t * (1 - c)), p)

    def expert(k):
        rows = cap
        for q in range(S // 2):
            for h in range(2):
                if q == 0 and h == 0:
                    @pl.when((k != 0) | (c != 0))
                    def _():
                        wait(r2.at[k, q, h], rcv.at[k, q, h])
                else:
                    wait(r2.at[k, q, h], rcv.at[k, q, h])
        for q in range(S // 2):
            xa = rcv[k, q, 0].astype(F32).reshape(rows, half)
            xb = rcv[k, q, 1].astype(F32).reshape(rows, half)
            squares = jnp.sum(xa * xa, axis=1, keepdims=True) + jnp.sum(xb * xb, axis=1, keepdims=True)
            scale = lax.rsqrt(squares * (1.0 / (2 * half)) + 1e-06)
            normed[q * rows : (q + 1) * rows, :half] = xa * scale * gain[:, :half]
            normed[q * rows : (q + 1) * rows, half:] = xb * scale * gain[:, half:]
        xn = normed[...].astype(BF16)
        hidden = []
        for i in range(2):
            gate = jnp.dot(xn, wg[i], preferred_element_type=F32)
            upper = jnp.dot(xn, wu[i], preferred_element_type=F32)
            hidden.append((gate / (1.0 + jnp.exp(-gate)) * upper).astype(BF16))
        hidden = jnp.concatenate(hidden, axis=1)
        for h in range(2):
            result = jnp.dot(hidden, wd[h], preferred_element_type=F32)
            result = result.reshape(S // 2, blocks, 8, half).astype(BF16)
            for q in range(S // 2):
                res[k, q, h] = result[q]
        for q in range(S // 2):
            dx = 2 * q + c
            dy = (dx + k) % S
            direct = (dx == 0) | (dy == 0)
            for h in range(2):
                j = dy if h else dx

                @pl.when(jnp.logical_not(direct))
                def _():
                    chip = at(0, -dy) if h else at(-dx, 0)
                    send(res.at[k, q, h], rl2.at[k, j], s_c.at[k, q, h], r3.at[k, j], chip, h)

                away = direct if h else direct & ((dx != 0) | (dy != 0))

                @pl.when(away)
                def _():
                    send(res.at[k, q, h], back.at[k, j], s_c.at[k, q, h], r4.at[k, j], at(-dx, -dy), h)

                if q == 0 and h == 0:
                    @pl.when((k == 0) & (c == 0))
                    def _():
                        back[0, 0] = res[0, 0, 0]

    def relay_return(k):
        for j in range(1, S):
            t, dx, dy = coords(j, k)

            @pl.when(t != 0)
            def _():
                wait(r3.at[k, j], rl2.at[k, j])
                send(rl2.at[k, j], back.at[k, j], s_d.at[k, j], r4.at[k, j], at(-t * c, -t * (1 - c)), c)

    def combine(k):
        for j in range(S):
            if j == 0:
                @pl.when((k != 0) | (c != 0))
                def _():
                    wait(r4.at[k, j], back.at[k, j])
            else:
                wait(r4.at[k, j], back.at[k, j])
        p = positions(k, (1, S * cap), 1)
        first = p == wts_hi_lo[:, 0:1]
        second = p == wts_hi_lo[:, 1:2]
        hi = jnp.where(first, wts_hi_lo[:, 2:3], jnp.where(second, wts_hi_lo[:, 3:4], 0.0)).astype(BF16)
        lo = jnp.where(first, wts_hi_lo[:, 4:5], jnp.where(second, wts_hi_lo[:, 5:6], 0.0)).astype(BF16)
        rows = back[k].astype(F32).reshape(S * cap, half).astype(BF16)
        acc[...] += jnp.dot(hi, rows, preferred_element_type=F32) + jnp.dot(lo, rows, preferred_element_type=F32)

    def loop(low, high, *steps):
        def body(k, _):
            for step in steps:
                step(k)
            return 0

        lax.fori_loop(low, high, body, 0)

    gather(0)
    pl.semaphore_wait(barrier, 4 * (S - 1) + 1)
    dispatch(0)
    for i, (src, dst) in enumerate(weights):
        send(src.at[0], dst.at[c], s_w.at[i], r_w.at[i], ep, 1 - c)
    loop(1, S, gather, dispatch)
    acc[...] = jnp.zeros_like(acc)
    ahead = min(2, S)
    loop(0, ahead, relay_dispatch)
    for i, (src, dst) in enumerate(weights):
        wait(l_w.at[i], dst.at[c])
        wait(r_w.at[i], dst.at[1 - c])

    def relay_and_expert(k):
        @pl.when(k + ahead < S)
        def _():
            relay_dispatch(k + ahead)

        expert(k)

    loop(0, S, relay_and_expert)

    def relay_and_combine(k):
        @pl.when(k < S)
        def _():
            relay_return(k)

        @pl.when(k >= ahead)
        def _():
            combine(k - ahead)

    loop(0, S + ahead, relay_and_combine)
    out[...] = acc[...].astype(BF16)

    def sent(k):
        for j in range(S):
            if j == 0:
                @pl.when((k != 0) | (c != 0))
                def _():
                    wait(s_a.at[k, j], snd.at[k, j])
            else:
                wait(s_a.at[k, j], snd.at[k, j])

                @pl.when((j + s * k + S) % S != 0)
                def _():
                    wait(s_b.at[k, j], rl1.at[k, j])
                    wait(s_d.at[k, j], rl2.at[k, j])
        for q in range(S // 2):
            for h in range(2):
                if q == 0 and h == 0:
                    @pl.when((k != 0) | (c != 0))
                    def _():
                        wait(s_c.at[k, q, h], res.at[k, q, h])
                else:
                    wait(s_c.at[k, q, h], res.at[k, q, h])

    loop(0, S, sent)
    for i, (src, dst) in enumerate(weights):
        wait(s_w.at[i], dst.at[c])


def on_device(tokens, norm_gain, expert_ids, route_weights, gate_weight, up_weight, down_weight):
    tok_rows, half = tokens.shape
    experts = lax.axis_size("ep")
    side = math.isqrt(experts)
    top = expert_ids.shape[1]
    cap = max(2, (3 * tok_rows * top + 2 * experts - 1) // (2 * experts))
    width, part = gate_weight.shape[1:]
    S = side
    block = (cap // 8, 8, half)
    vmem = pl.BlockSpec(memory_space=pltpu.VMEM)
    hbm = pl.BlockSpec(memory_space=pl.ANY)
    dma = pltpu.SemaphoreType.DMA
    return pl.pallas_call(
        functools.partial(kernel, side, cap),
        out_shape=jax.ShapeDtypeStruct((tok_rows, half), BF16),
        in_specs=[vmem] * 4 + [hbm] * 3,
        out_specs=vmem,
        scratch_shapes=[
            pltpu.VMEM((2, width, part), BF16),
            pltpu.VMEM((2, width, part), BF16),
            pltpu.VMEM((2, 2 * part, half), BF16),
            pltpu.VMEM((S, S) + block, BF16),
            pltpu.VMEM((S, S) + block, BF16),
            pltpu.VMEM((S, S // 2, 2) + block, BF16),
            pltpu.VMEM((S, S // 2, 2) + block, BF16),
            pltpu.VMEM((S, S) + block, BF16),
            pltpu.VMEM((S, S) + block, BF16),
            pltpu.VMEM((S // 2 * cap, width), F32),
            pltpu.VMEM((tok_rows, half), F32),
            pltpu.VMEM((8, tok_rows), F32),
            pltpu.VMEM((tok_rows, 128), F32),
            dma((3,)), dma((3,)), dma((3,)),
            dma((S, S)), dma((S, S)), dma((S, S // 2, 2)), dma((S, S)),
            dma((S, S)), dma((S, S // 2, 2)), dma((S, S)), dma((S, S)),
        ],
        compiler_params=pltpu.CompilerParams(
            collective_id=0, has_side_effects=True, vmem_limit_bytes=56 * 2**20
        ),
    )(tokens, norm_gain.reshape(1, -1), expert_ids.T, route_weights.T, gate_weight, up_weight, down_weight)


def solution(mesh):
    in_specs = (
        P(("grp", "ep"), "tp"),
        P(),
        P(("grp", "ep"), None),
        P(("grp", "ep"), None),
        P("ep", None, "tp"),
        P("ep", None, "tp"),
        P("ep", None, "tp"),
    )
    out_specs = P(("grp", "ep"), "tp")
    return jax.shard_map(
        on_device, mesh=mesh, in_specs=in_specs, out_specs=out_specs, check_vma=False
    )
```

```python
import functools
import math

import jax
import jax.numpy as jnp
from jax import lax
from jax.experimental import pallas as pl
from jax.experimental.pallas import tpu as pltpu
from jax.sharding import PartitionSpec as P

MESH = pl.DeviceIdType.MESH
BF16 = jnp.bfloat16
F32 = jnp.float32


def wrapped(v, side):
    v = jnp.where(v < 0, v + side, v)
    return jnp.where(v >= side, v - side, v)


def kernel(
    side, cap,
    tok_hbm, gain, ids, wts, gate_hbm, up_hbm, down_hbm, out,
    tok, wg, wu, wd, snd, rl1, rcv, res, rl2, back, normed, acc, posr, wts_hi_lo,
    s_w, r_w, l_w, l_t, s_a, s_b, s_c, s_d, r1, r2, r3, r3_last, r4,
):
    S = side
    half_side = S // 2
    c = lax.axis_index("tp")
    ep = lax.axis_index("ep")
    y = ep // S
    x = ep % S
    s = 1 - 2 * c
    tok_rows = tok.shape[0]
    half = tok.shape[1]
    blocks = cap // 8

    def at(dx, dy):
        return ((y + dy + S) % S) * S + (x + dx + S) % S

    def send(src, dst, send_sem, recv_sem, chip, core):
        pltpu.make_async_remote_copy(
            src_ref=src, dst_ref=dst, send_sem=send_sem, recv_sem=recv_sem,
            device_id={"ep": chip, "tp": core}, device_id_type=MESH,
        ).start()

    def wait(sem, ref):
        pltpu.make_async_copy(ref, ref, sem).wait()

    tok_copy = pltpu.make_async_copy(tok_hbm, tok, l_t)
    tok_copy.start()

    barrier = pltpu.get_barrier_semaphore()
    for d in range(1, S):
        for h in range(2):
            pl.semaphore_signal(barrier, inc=1, device_id={"ep": at(d, 0), "tp": h}, device_id_type=MESH)
            pl.semaphore_signal(barrier, inc=1, device_id={"ep": at(0, d), "tp": h}, device_id_type=MESH)
    pl.semaphore_signal(barrier, inc=1, device_id={"ep": ep, "tp": 1 - c}, device_id_type=MESH)

    weights = ((gate_hbm, wg), (up_hbm, wu), (down_hbm, wd))
    for i, (src, dst) in enumerate(weights):
        pltpu.make_async_copy(src.at[0], dst.at[c], l_w.at[i]).start()

    row = lax.broadcasted_iota(jnp.int32, (128, tok_rows), 0)
    e0 = ids[0:1, :]
    e1 = ids[1:2, :]
    hot0 = (row == e0).astype(F32)
    hot1 = (row == e1).astype(F32)
    earlier = (
        lax.broadcasted_iota(jnp.int32, (tok_rows, tok_rows), 0)
        < lax.broadcasted_iota(jnp.int32, (tok_rows, tok_rows), 1)
    )
    rank = jnp.dot(
        (hot0 + hot1).astype(BF16), earlier.astype(F32).astype(BF16), preferred_element_type=F32
    )
    pos0 = jnp.sum(rank * hot0, axis=0, keepdims=True) + (e0 * cap).astype(F32)
    pos1 = jnp.sum(rank * hot1, axis=0, keepdims=True) + (e1 * cap).astype(F32)
    posr[0:1, :] = pos0
    posr[1:2, :] = pos1

    def weight_table():
        w0 = wts[0:1, :]
        w1 = wts[1:2, :]
        w0_hi = w0.astype(BF16).astype(F32)
        w1_hi = w1.astype(BF16).astype(F32)
        row = lax.broadcasted_iota(jnp.int32, (128, tok_rows), 0)
        table = jnp.zeros((128, tok_rows), F32)
        columns = (posr[0:1, :], posr[1:2, :], w0_hi, w1_hi, w0 - w0_hi, w1 - w1_hi)
        for i, values in enumerate(columns):
            table = jnp.where(row == i, values, table)
        wts_hi_lo[...] = jnp.transpose(table)

    def coords(j, k):
        t = (j + s * k + S) % S
        return t, j * (1 - c) + t * c, j * c + t * (1 - c)

    def positions(k, i, low, count):
        j = jnp.zeros(i.shape, jnp.int32)
        for m in range(1, count):
            j = j + (i >= m * cap).astype(jnp.int32)
        slot = i - j * cap
        j = j + low
        t = wrapped(j + s * k, S)
        dx = jnp.where(c == 0, j, t)
        dy = jnp.where(c == 0, t, j)
        e = wrapped(y + dy, S) * S + wrapped(x + dx, S)
        return (e * cap + slot).astype(F32)

    def gather(k):
        p = positions(k, lax.broadcasted_iota(jnp.int32, (S * cap, 1), 0), 0, S)
        pick = jnp.where(p == posr[0:1, :], 1.0, jnp.where(p == posr[1:2, :], 1.0, 0.0))
        rows = jnp.dot(pick.astype(BF16), tok[...], preferred_element_type=F32)
        snd[k] = rows.reshape(S, blocks, 8, half).astype(BF16)

    def dispatch(k):
        for j in range(S):
            t, dx, dy = coords(j, k)
            p = dx % 2
            q = dx // 2
            if j == 0:
                @pl.when(t != 0)
                def _():
                    send(snd.at[k, j], rcv.at[k, q, c], s_a, r2.at[k], at(dx, dy), p)

                @pl.when((t == 0) & (c == 1))
                def _():
                    send(snd.at[k, j], rcv.at[k, q, c], s_a, r2.at[k], ep, 0)

                @pl.when((t == 0) & (c == 0))
                def _():
                    rcv[0, 0, 0] = snd[0, 0]
            else:
                @pl.when(t != 0)
                def _():
                    send(snd.at[k, j], rl1.at[k, j], s_a, r1.at[k], at(j * (1 - c), j * c), c)

                @pl.when(t == 0)
                def _():
                    send(snd.at[k, j], rcv.at[k, q, c], s_a, r2.at[k], at(dx, dy), p)

    def wait_blocks(sem, ref, count):
        wait(sem, ref.at[pl.ds(0, count)])

    def wait_relayed(sem, ref, k):
        @pl.when(k == 0)
        def _():
            wait_blocks(sem, ref.at[k], S - 1)

        if S > 2:
            @pl.when(k != 0)
            def _():
                wait_blocks(sem, ref.at[k], S - 2)

    def relay_dispatch(k):
        wait_relayed(r1.at[k], rl1, k)
        for j in range(1, S):
            t, dx, dy = coords(j, k)
            p = dx % 2
            q = dx // 2

            @pl.when(t != 0)
            def _():
                send(rl1.at[k, j], rcv.at[k, q, c], s_b, r2.at[k], at(t * c, t * (1 - c)), p)

    def send_relayed(k, j, src, chip, core):
        @pl.when(k == S - 1)
        def _():
            send(src, rl2.at[k, j], s_c, r3_last.at[j], chip, core)

        @pl.when(k != S - 1)
        def _():
            send(src, rl2.at[k, j], s_c, r3.at[k], chip, core)

    def expert(k):
        rows = cap
        own = (k == 0) & (c == 0)

        @pl.when(own)
        def _():
            wait_blocks(r2.at[k], back.at[k], S - 1)

        @pl.when(jnp.logical_not(own))
        def _():
            wait_blocks(r2.at[k], back.at[k], S)

        for q in range(S // 2):
            xa = rcv[k, q, 0].astype(F32).reshape(rows, half)
            xb = rcv[k, q, 1].astype(F32).reshape(rows, half)
            squares = jnp.sum(xa * xa, axis=1, keepdims=True) + jnp.sum(xb * xb, axis=1, keepdims=True)
            scale = lax.rsqrt(squares * (1.0 / (2 * half)) + 1e-06)
            normed[q * rows : (q + 1) * rows, :half] = xa * scale * gain[:, :half]
            normed[q * rows : (q + 1) * rows, half:] = xb * scale * gain[:, half:]
        xn = normed[...].astype(BF16)
        hidden = []
        for i in range(2):
            gate = jnp.dot(xn, wg[i], preferred_element_type=F32)
            upper = jnp.dot(xn, wu[i], preferred_element_type=F32)
            hidden.append((gate / (1.0 + jnp.exp(-gate)) * upper).astype(BF16))
        hidden = jnp.concatenate(hidden, axis=1)
        for h in range(2):
            result = jnp.dot(hidden, wd[h], preferred_element_type=F32)
            result = result.reshape(S // 2, blocks, 8, half).astype(BF16)
            for q in range(S // 2):
                res[k, q, h] = result[q]
        for q in range(S // 2):
            dx = 2 * q + c
            dy = (dx + k) % S
            direct = (dx == 0) | (dy == 0)
            for h in range(2):
                j = dy if h else dx

                @pl.when(jnp.logical_not(direct))
                def _():
                    chip = at(0, -dy) if h else at(-dx, 0)
                    send_relayed(k, j, res.at[k, q, h], chip, h)

                away = direct if h else direct & ((dx != 0) | (dy != 0))

                @pl.when(away)
                def _():
                    send(res.at[k, q, h], back.at[k, j], s_c, r4.at[k, j // half_side], at(-dx, -dy), h)

                if q == 0 and h == 0:
                    @pl.when((k == 0) & (c == 0))
                    def _():
                        back[0, 0] = res[0, 0, 0]

    def relay_return(k):
        @pl.when(k != S - 1)
        def _():
            wait_relayed(r3.at[k], rl2, k)

        for j in range(1, S):
            t, dx, dy = coords(j, k)

            @pl.when(t != 0)
            def _():
                @pl.when(k == S - 1)
                def _():
                    wait(r3_last.at[j], rl2.at[k, j])

                send(rl2.at[k, j], back.at[k, j], s_d, r4.at[k, j // half_side], at(-t * c, -t * (1 - c)), c)

    def combined(k, part):
        if part == 0:
            own = (k == 0) & (c == 0)

            @pl.when(own)
            def _():
                if half_side > 1:
                    wait_blocks(r4.at[k, part], back.at[k], half_side - 1)

            @pl.when(jnp.logical_not(own))
            def _():
                wait_blocks(r4.at[k, part], back.at[k], half_side)
        else:
            wait_blocks(r4.at[k, part], back.at[k], half_side)
        count = half_side * cap
        i = lax.broadcasted_iota(jnp.int32, (1, 2 * count), 1)
        high = i < count
        p = positions(k, jnp.where(high, i, i - count), part * half_side, half_side)
        one = jnp.where(high, wts_hi_lo[:, 2:3], wts_hi_lo[:, 4:5])
        two = jnp.where(high, wts_hi_lo[:, 3:4], wts_hi_lo[:, 5:6])
        mix = jnp.where(p == wts_hi_lo[:, 0:1], one, jnp.where(p == wts_hi_lo[:, 1:2], two, 0.0))
        rows = back[k, part * half_side : (part + 1) * half_side].astype(F32).reshape(count, half)
        rows = jnp.concatenate([rows, rows], axis=0).astype(BF16)
        return jnp.dot(mix.astype(BF16), rows, preferred_element_type=F32)

    def combine(k):
        for part in range(2):
            acc[...] += combined(k, part)

    def loop(low, high, *steps):
        def body(k, _):
            for step in steps:
                step(k)
            return 0

        lax.fori_loop(low, high, body, 0)

    tok_copy.wait()
    gather(0)
    pl.semaphore_wait(barrier, 4 * (S - 1) + 1)
    dispatch(0)
    for i, (src, dst) in enumerate(weights):
        send(src.at[0], dst.at[c], s_w.at[i], r_w.at[i], ep, 1 - c)
    loop(1, S, gather, dispatch)
    weight_table()
    acc[...] = jnp.zeros_like(acc)
    ahead = min(2, S)
    loop(0, ahead, relay_dispatch)
    for i, (src, dst) in enumerate(weights):
        wait(l_w.at[i], dst.at[c])
        wait(r_w.at[i], dst.at[1 - c])

    def relay_and_expert(k):
        @pl.when(k + ahead < S)
        def _():
            relay_dispatch(k + ahead)

        expert(k)

    loop(0, S, relay_and_expert)

    def relay_and_combine(k):
        @pl.when(k < S)
        def _():
            relay_return(k)

        @pl.when(k >= ahead)
        def _():
            combine(k - ahead)

    loop(0, S + ahead - 1, relay_and_combine)
    acc[...] += combined(S - 1, 0)
    out[...] = (acc[...] + combined(S - 1, 1)).astype(BF16)

    blocks_sent = S * S
    relayed = S - 1 + (S - 1) * (S - 2)

    def all_sent(sem, count):
        rows = count // S
        wait(sem, snd.at[pl.ds(0, rows)])
        if count % S:
            wait(sem, snd.at[0, pl.ds(0, count % S)])

    for sem in (s_a, s_c):
        @pl.when(c == 0)
        def _():
            all_sent(sem, blocks_sent - 1)

        @pl.when(c != 0)
        def _():
            all_sent(sem, blocks_sent)
    for sem in (s_b, s_d):
        all_sent(sem, relayed)
    for i, (src, dst) in enumerate(weights):
        wait(s_w.at[i], dst.at[c])


def on_device(tokens, norm_gain, expert_ids, route_weights, gate_weight, up_weight, down_weight):
    tok_rows, half = tokens.shape
    experts = lax.axis_size("ep")
    side = math.isqrt(experts)
    top = expert_ids.shape[1]
    cap = max(2, (3 * tok_rows * top + 2 * experts - 1) // (2 * experts))
    width, part = gate_weight.shape[1:]
    S = side
    block = (cap // 8, 8, half)
    vmem = pl.BlockSpec(memory_space=pltpu.VMEM)
    hbm = pl.BlockSpec(memory_space=pltpu.HBM)
    dma = pltpu.SemaphoreType.DMA
    return pl.pallas_call(
        functools.partial(kernel, side, cap),
        out_shape=jax.ShapeDtypeStruct((tok_rows, half), BF16),
        in_specs=[hbm] + [vmem] * 3 + [hbm] * 3,
        out_specs=vmem,
        scratch_shapes=[
            pltpu.VMEM((tok_rows, half), BF16),
            pltpu.VMEM((2, width, part), BF16),
            pltpu.VMEM((2, width, part), BF16),
            pltpu.VMEM((2, 2 * part, half), BF16),
            pltpu.VMEM((S, S) + block, BF16),
            pltpu.VMEM((S, S) + block, BF16),
            pltpu.VMEM((S, S // 2, 2) + block, BF16),
            pltpu.VMEM((S, S // 2, 2) + block, BF16),
            pltpu.VMEM((S, S) + block, BF16),
            pltpu.VMEM((S, S) + block, BF16),
            pltpu.VMEM((S // 2 * cap, width), F32),
            pltpu.VMEM((tok_rows, half), F32),
            pltpu.VMEM((8, tok_rows), F32),
            pltpu.VMEM((tok_rows, 128), F32),
            dma((3,)), dma((3,)), dma((3,)), dma,
            dma, dma, dma, dma,
            dma((S,)), dma((S,)), dma((S,)), dma((S,)), dma((S, 2)),
        ],
        compiler_params=pltpu.CompilerParams(
            collective_id=0, has_side_effects=True, vmem_limit_bytes=52 * 2**20
        ),
    )(tokens, norm_gain.reshape(1, -1), expert_ids.T, route_weights.T, gate_weight, up_weight, down_weight)


def solution(mesh):
    in_specs = (
        P(("grp", "ep"), "tp"),
        P(),
        P(("grp", "ep"), None),
        P(("grp", "ep"), None),
        P("ep", None, "tp"),
        P("ep", None, "tp"),
        P("ep", None, "tp"),
    )
    out_specs = P(("grp", "ep"), "tp")
    return jax.shard_map(
        on_device, mesh=mesh, in_specs=in_specs, out_specs=out_specs, check_vma=False
    )
```

```python
import functools
import math

import jax
import jax.numpy as jnp
from jax import lax
from jax.experimental import pallas as pl
from jax.experimental.pallas import tpu as pltpu
from jax.sharding import PartitionSpec as P

MESH = pl.DeviceIdType.MESH
BF16 = jnp.bfloat16
F32 = jnp.float32


def wrapped(v, side):
    v = jnp.where(v < 0, v + side, v)
    return jnp.where(v >= side, v - side, v)


def kernel(
    side, cap,
    tok_hbm, gain, ids, wts, gate_hbm, up_hbm, down_hbm, out,
    tok, wg, wu, wd, snd, rl1, rcv, res, rl2, back, normed, acc, posr, wts_hi_lo,
    s_w, r_w, l_w, l_t, go, s_a, s_b, s_c, s_d, r1, r2, r3, r3_last, r4,
):
    S = side
    half_side = S // 2
    c = lax.axis_index("tp")
    ep = lax.axis_index("ep")
    y = ep // S
    x = ep % S
    s = 1 - 2 * c
    tok_rows = tok.shape[0]
    half = tok.shape[1]
    blocks = cap // 8

    def at(dx, dy):
        return ((y + dy + S) % S) * S + (x + dx + S) % S

    def send(src, dst, send_sem, recv_sem, chip, core):
        pltpu.make_async_remote_copy(
            src_ref=src, dst_ref=dst, send_sem=send_sem, recv_sem=recv_sem,
            device_id={"ep": chip, "tp": core}, device_id_type=MESH,
        ).start()

    def wait(sem, ref):
        pltpu.make_async_copy(ref, ref, sem).wait()

    tok_copy = pltpu.make_async_copy(tok_hbm, tok, l_t)
    tok_copy.start()

    barrier = pltpu.get_barrier_semaphore()
    for d in range(1, S):
        pl.semaphore_signal(barrier, inc=1, device_id={"ep": at(d, 0), "tp": c}, device_id_type=MESH)
        pl.semaphore_signal(barrier, inc=1, device_id={"ep": at(0, d), "tp": c}, device_id_type=MESH)
    pl.semaphore_signal(barrier, inc=1, device_id={"ep": ep, "tp": 1 - c}, device_id_type=MESH)

    weights = ((gate_hbm, wg), (up_hbm, wu), (down_hbm, wd))
    for i, (src, dst) in enumerate(weights):
        pltpu.make_async_copy(src.at[0], dst.at[c], l_w.at[i]).start()

    row = lax.broadcasted_iota(jnp.int32, (128, tok_rows), 0)
    e0 = ids[0:1, :]
    e1 = ids[1:2, :]
    hot0 = (row == e0).astype(F32)
    hot1 = (row == e1).astype(F32)
    earlier = (
        lax.broadcasted_iota(jnp.int32, (tok_rows, tok_rows), 0)
        < lax.broadcasted_iota(jnp.int32, (tok_rows, tok_rows), 1)
    )
    rank = jnp.dot(
        (hot0 + hot1).astype(BF16), earlier.astype(F32).astype(BF16), preferred_element_type=F32
    )
    pos0 = jnp.sum(rank * hot0, axis=0, keepdims=True) + (e0 * cap).astype(F32)
    pos1 = jnp.sum(rank * hot1, axis=0, keepdims=True) + (e1 * cap).astype(F32)
    posr[0:1, :] = pos0
    posr[1:2, :] = pos1

    def weight_table():
        w0 = wts[0:1, :]
        w1 = wts[1:2, :]
        w0_hi = w0.astype(BF16).astype(F32)
        w1_hi = w1.astype(BF16).astype(F32)
        row = lax.broadcasted_iota(jnp.int32, (128, tok_rows), 0)
        table = jnp.zeros((128, tok_rows), F32)
        columns = (posr[0:1, :], posr[1:2, :], w0_hi, w1_hi, w0 - w0_hi, w1 - w1_hi)
        for i, values in enumerate(columns):
            table = jnp.where(row == i, values, table)
        wts_hi_lo[...] = jnp.transpose(table)

    def coords(j, k):
        t = (j + s * k + S) % S
        return t, j * (1 - c) + t * c, j * c + t * (1 - c)

    def positions(k, i, low, count):
        j = jnp.zeros(i.shape, jnp.int32)
        for m in range(1, count):
            j = j + (i >= m * cap).astype(jnp.int32)
        slot = i - j * cap
        j = j + low
        t = wrapped(j + s * k, S)
        dx = jnp.where(c == 0, j, t)
        dy = jnp.where(c == 0, t, j)
        e = wrapped(y + dy, S) * S + wrapped(x + dx, S)
        return (e * cap + slot).astype(F32)

    def gather(k):
        p = positions(k, lax.broadcasted_iota(jnp.int32, (S * cap, 1), 0), 0, S)
        pick = jnp.where(p == posr[0:1, :], 1.0, jnp.where(p == posr[1:2, :], 1.0, 0.0))
        rows = jnp.dot(pick.astype(BF16), tok[...], preferred_element_type=F32)
        snd[k] = rows.reshape(S, blocks, 8, half).astype(BF16)

    def dispatch(k, crossing):
        for j in range(S):
            t, dx, dy = coords(j, k)
            p = dx % 2
            q = dx // 2
            now = (p != c) if crossing else (p == c)
            if j == 0:
                @pl.when(now & (t != 0))
                def _():
                    send(snd.at[k, j], rcv.at[k, q, c], s_a, r2.at[k], at(dx, dy), p)

                if not crossing:
                    @pl.when((t == 0) & (c == 1))
                    def _():
                        send(snd.at[k, j], rcv.at[k, q, c], s_a, r2.at[k], ep, 0)

                    @pl.when((t == 0) & (c == 0))
                    def _():
                        rcv[0, 0, 0] = snd[0, 0]
            else:
                if not crossing:
                    @pl.when(t != 0)
                    def _():
                        send(snd.at[k, j], rl1.at[k, j], s_a, r1.at[k], at(j * (1 - c), j * c), c)

                @pl.when(now & (t == 0))
                def _():
                    send(snd.at[k, j], rcv.at[k, q, c], s_a, r2.at[k], at(dx, dy), p)

    def dispatch_same(k):
        dispatch(k, False)

    def dispatch_crossing(k):
        dispatch(k, True)

    def wait_blocks(sem, ref, count):
        wait(sem, ref.at[pl.ds(0, count)])

    def wait_relayed(sem, ref, k):
        @pl.when(k == 0)
        def _():
            wait_blocks(sem, ref.at[k], S - 1)

        if S > 2:
            @pl.when(k != 0)
            def _():
                wait_blocks(sem, ref.at[k], S - 2)

    def relay_dispatch(k):
        wait_relayed(r1.at[k], rl1, k)
        for j in range(1, S):
            t, dx, dy = coords(j, k)
            p = dx % 2
            q = dx // 2

            @pl.when(t != 0)
            def _():
                send(rl1.at[k, j], rcv.at[k, q, c], s_b, r2.at[k], at(t * c, t * (1 - c)), p)

    def send_relayed(k, j, src, chip, core):
        @pl.when(k == S - 1)
        def _():
            send(src, rl2.at[k, j], s_c, r3_last.at[j], chip, core)

        @pl.when(k != S - 1)
        def _():
            send(src, rl2.at[k, j], s_c, r3.at[k], chip, core)

    def expert(k):
        rows = cap
        own = (k == 0) & (c == 0)

        @pl.when(own)
        def _():
            wait_blocks(r2.at[k], back.at[k], S - 1)

        @pl.when(jnp.logical_not(own))
        def _():
            wait_blocks(r2.at[k], back.at[k], S)

        for q in range(S // 2):
            xa = rcv[k, q, 0].astype(F32).reshape(rows, half)
            xb = rcv[k, q, 1].astype(F32).reshape(rows, half)
            squares = jnp.sum(xa * xa, axis=1, keepdims=True) + jnp.sum(xb * xb, axis=1, keepdims=True)
            scale = lax.rsqrt(squares * (1.0 / (2 * half)) + 1e-06)
            normed[q * rows : (q + 1) * rows, :half] = xa * scale * gain[:, :half]
            normed[q * rows : (q + 1) * rows, half:] = xb * scale * gain[:, half:]
        xn = normed[...].astype(BF16)
        hidden = []
        for i in range(2):
            gate = jnp.dot(xn, wg[i], preferred_element_type=F32)
            upper = jnp.dot(xn, wu[i], preferred_element_type=F32)
            hidden.append((gate / (1.0 + jnp.exp(-gate)) * upper).astype(BF16))
        hidden = jnp.concatenate(hidden, axis=1)
        for h in range(2):
            result = jnp.dot(hidden, wd[h], preferred_element_type=F32)
            result = result.reshape(S // 2, blocks, 8, half).astype(BF16)
            for q in range(S // 2):
                res[k, q, h] = result[q]
        for q in range(S // 2):
            dx = 2 * q + c
            dy = (dx + k) % S
            direct = (dx == 0) | (dy == 0)
            for h in range(2):
                j = dy if h else dx

                @pl.when(jnp.logical_not(direct))
                def _():
                    chip = at(0, -dy) if h else at(-dx, 0)
                    send_relayed(k, j, res.at[k, q, h], chip, h)

                away = direct if h else direct & ((dx != 0) | (dy != 0))

                @pl.when(away)
                def _():
                    send(res.at[k, q, h], back.at[k, j], s_c, r4.at[k, j // half_side], at(-dx, -dy), h)

                if q == 0 and h == 0:
                    @pl.when((k == 0) & (c == 0))
                    def _():
                        back[0, 0] = res[0, 0, 0]

    def relay_return(k):
        @pl.when(k != S - 1)
        def _():
            wait_relayed(r3.at[k], rl2, k)

        for j in range(1, S):
            t, dx, dy = coords(j, k)

            @pl.when(t != 0)
            def _():
                @pl.when(k == S - 1)
                def _():
                    wait(r3_last.at[j], rl2.at[k, j])

                send(rl2.at[k, j], back.at[k, j], s_d, r4.at[k, j // half_side], at(-t * c, -t * (1 - c)), c)

    def combined(k, part):
        if part == 0:
            own = (k == 0) & (c == 0)

            @pl.when(own)
            def _():
                if half_side > 1:
                    wait_blocks(r4.at[k, part], back.at[k], half_side - 1)

            @pl.when(jnp.logical_not(own))
            def _():
                wait_blocks(r4.at[k, part], back.at[k], half_side)
        else:
            wait_blocks(r4.at[k, part], back.at[k], half_side)
        count = half_side * cap
        i = lax.broadcasted_iota(jnp.int32, (1, 2 * count), 1)
        high = i < count
        p = positions(k, jnp.where(high, i, i - count), part * half_side, half_side)
        one = jnp.where(high, wts_hi_lo[:, 2:3], wts_hi_lo[:, 4:5])
        two = jnp.where(high, wts_hi_lo[:, 3:4], wts_hi_lo[:, 5:6])
        mix = jnp.where(p == wts_hi_lo[:, 0:1], one, jnp.where(p == wts_hi_lo[:, 1:2], two, 0.0))
        rows = back[k, part * half_side : (part + 1) * half_side].astype(F32).reshape(count, half)
        rows = jnp.concatenate([rows, rows], axis=0).astype(BF16)
        return jnp.dot(mix.astype(BF16), rows, preferred_element_type=F32)

    def combine(k):
        for part in range(2):
            acc[...] += combined(k, part)

    def loop(low, high, *steps):
        def body(k, _):
            for step in steps:
                step(k)
            return 0

        lax.fori_loop(low, high, body, 0)

    tok_copy.wait()
    gather(0)
    pl.semaphore_wait(barrier, 2 * (S - 1) + 1)
    pl.semaphore_signal(go, inc=1, device_id={"ep": ep, "tp": 1 - c}, device_id_type=MESH)
    dispatch_same(0)
    for i, (src, dst) in enumerate(weights):
        send(src.at[0], dst.at[c], s_w.at[i], r_w.at[i], ep, 1 - c)
    loop(1, S, gather, dispatch_same)
    pl.semaphore_wait(go, 1)
    loop(0, S, dispatch_crossing)
    weight_table()
    acc[...] = jnp.zeros_like(acc)
    ahead = min(2, S)
    loop(0, ahead, relay_dispatch)
    for i, (src, dst) in enumerate(weights):
        wait(l_w.at[i], dst.at[c])
        wait(r_w.at[i], dst.at[1 - c])

    def relay_and_expert(k):
        @pl.when(k + ahead < S)
        def _():
            relay_dispatch(k + ahead)

        expert(k)

    loop(0, S, relay_and_expert)

    def relay_and_combine(k):
        @pl.when(k < S)
        def _():
            relay_return(k)

        @pl.when(k >= ahead)
        def _():
            combine(k - ahead)

    loop(0, S + ahead - 1, relay_and_combine)
    acc[...] += combined(S - 1, 0)
    out[...] = (acc[...] + combined(S - 1, 1)).astype(BF16)

    blocks_sent = S * S
    relayed = S - 1 + (S - 1) * (S - 2)

    def all_sent(sem, count):
        rows = count // S
        wait(sem, snd.at[pl.ds(0, rows)])
        if count % S:
            wait(sem, snd.at[0, pl.ds(0, count % S)])

    for sem in (s_a, s_c):
        @pl.when(c == 0)
        def _():
            all_sent(sem, blocks_sent - 1)

        @pl.when(c != 0)
        def _():
            all_sent(sem, blocks_sent)
    for sem in (s_b, s_d):
        all_sent(sem, relayed)
    for i, (src, dst) in enumerate(weights):
        wait(s_w.at[i], dst.at[c])


def on_device(tokens, norm_gain, expert_ids, route_weights, gate_weight, up_weight, down_weight):
    tok_rows, half = tokens.shape
    experts = lax.axis_size("ep")
    side = math.isqrt(experts)
    top = expert_ids.shape[1]
    cap = max(2, (3 * tok_rows * top + 2 * experts - 1) // (2 * experts))
    width, part = gate_weight.shape[1:]
    S = side
    block = (cap // 8, 8, half)
    vmem = pl.BlockSpec(memory_space=pltpu.VMEM)
    hbm = pl.BlockSpec(memory_space=pltpu.HBM)
    dma = pltpu.SemaphoreType.DMA
    return pl.pallas_call(
        functools.partial(kernel, side, cap),
        out_shape=jax.ShapeDtypeStruct((tok_rows, half), BF16),
        in_specs=[hbm] + [vmem] * 3 + [hbm] * 3,
        out_specs=vmem,
        scratch_shapes=[
            pltpu.VMEM((tok_rows, half), BF16),
            pltpu.VMEM((2, width, part), BF16),
            pltpu.VMEM((2, width, part), BF16),
            pltpu.VMEM((2, 2 * part, half), BF16),
            pltpu.VMEM((S, S) + block, BF16),
            pltpu.VMEM((S, S) + block, BF16),
            pltpu.VMEM((S, S // 2, 2) + block, BF16),
            pltpu.VMEM((S, S // 2, 2) + block, BF16),
            pltpu.VMEM((S, S) + block, BF16),
            pltpu.VMEM((S, S) + block, BF16),
            pltpu.VMEM((S // 2 * cap, width), F32),
            pltpu.VMEM((tok_rows, half), F32),
            pltpu.VMEM((8, tok_rows), F32),
            pltpu.VMEM((tok_rows, 128), F32),
            dma((3,)), dma((3,)), dma((3,)), dma, pltpu.SemaphoreType.REGULAR,
            dma, dma, dma, dma,
            dma((S,)), dma((S,)), dma((S,)), dma((S,)), dma((S, 2)),
        ],
        compiler_params=pltpu.CompilerParams(
            collective_id=0, has_side_effects=True, vmem_limit_bytes=52 * 2**20
        ),
    )(tokens, norm_gain.reshape(1, -1), expert_ids.T, route_weights.T, gate_weight, up_weight, down_weight)


def solution(mesh):
    in_specs = (
        P(("grp", "ep"), "tp"),
        P(),
        P(("grp", "ep"), None),
        P(("grp", "ep"), None),
        P("ep", None, "tp"),
        P("ep", None, "tp"),
        P("ep", None, "tp"),
    )
    out_specs = P(("grp", "ep"), "tp")
    return jax.shard_map(
        on_device, mesh=mesh, in_specs=in_specs, out_specs=out_specs, check_vma=False
    )
```

```python
import functools
import math

import jax
import jax.numpy as jnp
from jax import lax
from jax.experimental import pallas as pl
from jax.experimental.pallas import tpu as pltpu
from jax.sharding import PartitionSpec as P

MESH = pl.DeviceIdType.MESH
BF16 = jnp.bfloat16
F32 = jnp.float32


def wrapped(v, side):
    v = jnp.where(v < 0, v + side, v)
    return jnp.where(v >= side, v - side, v)


def kernel(
    side, cap,
    tok_hbm, gain, ids, wts, gate_hbm, up_hbm, down_hbm, out,
    tok, wg, wu, wd, snd, rl1, rcv, res, rl2, back, normed, acc, posr, wts_hi_lo,
    s_w, r_w, l_w, l_t, go, s_a, s_b, s_c, s_d, r1, r2, r3, r3_last, r4,
):
    S = side
    half_side = S // 2
    c = lax.axis_index("tp")
    ep = lax.axis_index("ep")
    y = ep // S
    x = ep % S
    tok_rows = tok.shape[0]
    half = tok.shape[1]
    blocks = cap // 8

    def at(dx, dy):
        return ((y + dy + S) % S) * S + (x + dx + S) % S

    def send(src, dst, send_sem, recv_sem, chip, core):
        pltpu.make_async_remote_copy(
            src_ref=src, dst_ref=dst, send_sem=send_sem, recv_sem=recv_sem,
            device_id={"ep": chip, "tp": core}, device_id_type=MESH,
        ).start()

    def wait(sem, ref):
        pltpu.make_async_copy(ref, ref, sem).wait()

    tok_copy = pltpu.make_async_copy(tok_hbm, tok, l_t)
    tok_copy.start()

    barrier = pltpu.get_barrier_semaphore()
    for d in range(1, S):
        pl.semaphore_signal(barrier, inc=1, device_id={"ep": at(d, 0), "tp": c}, device_id_type=MESH)
        pl.semaphore_signal(barrier, inc=1, device_id={"ep": at(0, d), "tp": c}, device_id_type=MESH)
    pl.semaphore_signal(barrier, inc=1, device_id={"ep": ep, "tp": 1 - c}, device_id_type=MESH)

    weights = ((gate_hbm, wg), (up_hbm, wu), (down_hbm, wd))
    row = lax.broadcasted_iota(jnp.int32, (128, tok_rows), 0)
    e0 = ids[0:1, :]
    e1 = ids[1:2, :]
    hot0 = (row == e0).astype(F32)
    hot1 = (row == e1).astype(F32)
    earlier = (
        lax.broadcasted_iota(jnp.int32, (tok_rows, tok_rows), 0)
        < lax.broadcasted_iota(jnp.int32, (tok_rows, tok_rows), 1)
    )
    rank = jnp.dot(
        (hot0 + hot1).astype(BF16), earlier.astype(F32).astype(BF16), preferred_element_type=F32
    )
    pos0 = jnp.sum(rank * hot0, axis=0, keepdims=True) + (e0 * cap).astype(F32)
    pos1 = jnp.sum(rank * hot1, axis=0, keepdims=True) + (e1 * cap).astype(F32)
    posr[0:1, :] = pos0
    posr[1:2, :] = pos1

    def weight_table():
        w0 = wts[0:1, :]
        w1 = wts[1:2, :]
        w0_hi = w0.astype(BF16).astype(F32)
        w1_hi = w1.astype(BF16).astype(F32)
        row = lax.broadcasted_iota(jnp.int32, (128, tok_rows), 0)
        table = jnp.zeros((128, tok_rows), F32)
        columns = (posr[0:1, :], posr[1:2, :], w0_hi, w1_hi, w0 - w0_hi, w1 - w1_hi)
        for i, values in enumerate(columns):
            table = jnp.where(row == i, values, table)
        wts_hi_lo[...] = jnp.transpose(table)

    def first_axis(core, k):
        return (core + k) % 2

    def coords(j, k):
        f = first_axis(c, k)
        t = (j + (1 - 2 * f) * k + S) % S
        return t, j * (1 - f) + t * f, j * f + t * (1 - f)

    def positions(k, i, low, count):
        j = jnp.zeros(i.shape, jnp.int32)
        for m in range(1, count):
            j = j + (i >= m * cap).astype(jnp.int32)
        slot = i - j * cap
        j = j + low
        f = first_axis(c, k)
        t = wrapped(j + (1 - 2 * f) * k, S)
        dx = jnp.where(f == 0, j, t)
        dy = jnp.where(f == 0, t, j)
        e = wrapped(y + dy, S) * S + wrapped(x + dx, S)
        return (e * cap + slot).astype(F32)

    def gather(k):
        p = positions(k, lax.broadcasted_iota(jnp.int32, (S * cap, 1), 0), 0, S)
        pick = jnp.where(p == posr[0:1, :], 1.0, jnp.where(p == posr[1:2, :], 1.0, 0.0))
        rows = jnp.dot(pick.astype(BF16), tok[...], preferred_element_type=F32)
        snd[k] = rows.reshape(S, blocks, 8, half).astype(BF16)

    def dispatch(k, crossing):
        f = first_axis(c, k)
        for j in range(S):
            t, dx, dy = coords(j, k)
            p = dx % 2
            q = dx // 2
            now = (p != c) if crossing else (p == c)
            if j == 0:
                @pl.when(now & (t != 0))
                def _():
                    send(snd.at[k, j], rcv.at[k, q, c], s_a, r2.at[k], at(dx, dy), p)

                if not crossing:
                    @pl.when((t == 0) & (c == 1))
                    def _():
                        send(snd.at[k, j], rcv.at[k, q, c], s_a, r2.at[k], ep, 0)

                    @pl.when((t == 0) & (c == 0))
                    def _():
                        rcv[0, 0, 0] = snd[0, 0]
            else:
                if not crossing:
                    @pl.when(t != 0)
                    def _():
                        send(snd.at[k, j], rl1.at[k, j], s_a, r1.at[k], at(j * (1 - f), j * f), c)

                @pl.when(now & (t == 0))
                def _():
                    send(snd.at[k, j], rcv.at[k, q, c], s_a, r2.at[k], at(dx, dy), p)

    def dispatch_same(k):
        dispatch(k, False)

    def dispatch_crossing(k):
        dispatch(k, True)

    def wait_blocks(sem, ref, count):
        wait(sem, ref.at[pl.ds(0, count)])

    def wait_relayed(sem, ref, k):
        @pl.when(k == 0)
        def _():
            wait_blocks(sem, ref.at[k], S - 1)

        if S > 2:
            @pl.when(k != 0)
            def _():
                wait_blocks(sem, ref.at[k], S - 2)

    def relay_dispatch(k):
        wait_relayed(r1.at[k], rl1, k)
        f = first_axis(c, k)
        for j in range(1, S):
            t, dx, dy = coords(j, k)
            p = dx % 2
            q = dx // 2

            @pl.when(t != 0)
            def _():
                send(rl1.at[k, j], rcv.at[k, q, c], s_b, r2.at[k], at(t * f, t * (1 - f)), p)

    def send_relayed(k, j, src, chip, core):
        @pl.when(k == S - 1)
        def _():
            send(src, rl2.at[k, j], s_c, r3_last.at[j], chip, core)

        @pl.when(k != S - 1)
        def _():
            send(src, rl2.at[k, j], s_c, r3.at[k], chip, core)

    def expert(k):
        rows = cap
        own = (k == 0) & (c == 0)

        @pl.when(own)
        def _():
            wait_blocks(r2.at[k], back.at[k], S - 1)

        @pl.when(jnp.logical_not(own))
        def _():
            wait_blocks(r2.at[k], back.at[k], S)

        for q in range(S // 2):
            xa = rcv[k, q, 0].astype(F32).reshape(rows, half)
            xb = rcv[k, q, 1].astype(F32).reshape(rows, half)
            squares = jnp.sum(xa * xa, axis=1, keepdims=True) + jnp.sum(xb * xb, axis=1, keepdims=True)
            scale = lax.rsqrt(squares * (1.0 / (2 * half)) + 1e-06)
            normed[q * rows : (q + 1) * rows, :half] = xa * scale * gain[:, :half]
            normed[q * rows : (q + 1) * rows, half:] = xb * scale * gain[:, half:]
        xn = normed[...].astype(BF16)
        hidden = []
        for i in range(2):
            gate = jnp.dot(xn, wg[i], preferred_element_type=F32)
            upper = jnp.dot(xn, wu[i], preferred_element_type=F32)
            hidden.append((gate / (1.0 + jnp.exp(-gate)) * upper).astype(BF16))
        hidden = jnp.concatenate(hidden, axis=1)
        for h in range(2):
            result = jnp.dot(hidden, wd[h], preferred_element_type=F32)
            result = result.reshape(S // 2, blocks, 8, half).astype(BF16)
            for q in range(S // 2):
                res[k, q, h] = result[q]
        for q in range(S // 2):
            dx = 2 * q + c
            dy = (dx + k) % S
            direct = (dx == 0) | (dy == 0)
            for h in range(2):
                f = first_axis(h, k)
                j = dx * (1 - f) + dy * f

                @pl.when(jnp.logical_not(direct))
                def _():
                    send_relayed(k, j, res.at[k, q, h], at(-dx * (1 - f), -dy * f), h)

                away = direct if h else direct & ((dx != 0) | (dy != 0))

                @pl.when(away)
                def _():
                    send(res.at[k, q, h], back.at[k, j], s_c, r4.at[k, j // half_side], at(-dx, -dy), h)

                if q == 0 and h == 0:
                    @pl.when((k == 0) & (c == 0))
                    def _():
                        back[0, 0] = res[0, 0, 0]

    def relay_return(k):
        f = first_axis(c, k)

        @pl.when(k != S - 1)
        def _():
            wait_relayed(r3.at[k], rl2, k)

        for j in range(1, S):
            t, dx, dy = coords(j, k)

            @pl.when(t != 0)
            def _():
                @pl.when(k == S - 1)
                def _():
                    wait(r3_last.at[j], rl2.at[k, j])

                send(rl2.at[k, j], back.at[k, j], s_d, r4.at[k, j // half_side], at(-t * f, -t * (1 - f)), c)

    def combined(k, part):
        if part == 0:
            own = (k == 0) & (c == 0)

            @pl.when(own)
            def _():
                if half_side > 1:
                    wait_blocks(r4.at[k, part], back.at[k], half_side - 1)

            @pl.when(jnp.logical_not(own))
            def _():
                wait_blocks(r4.at[k, part], back.at[k], half_side)
        else:
            wait_blocks(r4.at[k, part], back.at[k], half_side)
        count = half_side * cap
        i = lax.broadcasted_iota(jnp.int32, (1, 2 * count), 1)
        high = i < count
        p = positions(k, jnp.where(high, i, i - count), part * half_side, half_side)
        one = jnp.where(high, wts_hi_lo[:, 2:3], wts_hi_lo[:, 4:5])
        two = jnp.where(high, wts_hi_lo[:, 3:4], wts_hi_lo[:, 5:6])
        mix = jnp.where(p == wts_hi_lo[:, 0:1], one, jnp.where(p == wts_hi_lo[:, 1:2], two, 0.0))
        rows = back[k, part * half_side : (part + 1) * half_side].astype(F32).reshape(count, half)
        rows = jnp.concatenate([rows, rows], axis=0).astype(BF16)
        return jnp.dot(mix.astype(BF16), rows, preferred_element_type=F32)

    def combine(k):
        for part in range(2):
            acc[...] += combined(k, part)

    def loop(low, high, *steps):
        def body(k, _):
            for step in steps:
                step(k)
            return 0

        lax.fori_loop(low, high, body, 0)

    tok_copy.wait()
    gather(0)
    pl.semaphore_wait(barrier, 2 * (S - 1) + 1)
    pl.semaphore_signal(go, inc=1, device_id={"ep": ep, "tp": 1 - c}, device_id_type=MESH)
    dispatch_same(0)
    loop(1, S, gather, dispatch_same)
    for i, (src, dst) in enumerate(weights):
        send(src.at[0], dst.at[c], s_w.at[i], r_w.at[i], ep, 1 - c)
        pltpu.make_async_copy(src.at[0], dst.at[c], l_w.at[i]).start()
    pl.semaphore_wait(go, 1)
    loop(0, S, dispatch_crossing)
    weight_table()
    acc[...] = jnp.zeros_like(acc)
    ahead = min(3, S)
    loop(0, ahead, relay_dispatch)
    for i, (src, dst) in enumerate(weights):
        wait(l_w.at[i], dst.at[c])
        wait(r_w.at[i], dst.at[1 - c])

    def relay_and_expert(k):
        @pl.when(k + ahead < S)
        def _():
            relay_dispatch(k + ahead)

        expert(k)

    loop(0, S, relay_and_expert)

    def relay_and_combine(k):
        @pl.when(k < S)
        def _():
            relay_return(k)

        @pl.when(k >= ahead)
        def _():
            combine(k - ahead)

    loop(0, S + ahead - 1, relay_and_combine)
    acc[...] += combined(S - 1, 0)
    out[...] = (acc[...] + combined(S - 1, 1)).astype(BF16)

    blocks_sent = S * S
    relayed = S - 1 + (S - 1) * (S - 2)

    def all_sent(sem, count):
        rows = count // S
        wait(sem, snd.at[pl.ds(0, rows)])
        if count % S:
            wait(sem, snd.at[0, pl.ds(0, count % S)])

    for sem in (s_a, s_c):
        @pl.when(c == 0)
        def _():
            all_sent(sem, blocks_sent - 1)

        @pl.when(c != 0)
        def _():
            all_sent(sem, blocks_sent)
    for sem in (s_b, s_d):
        all_sent(sem, relayed)
    for i, (src, dst) in enumerate(weights):
        wait(s_w.at[i], dst.at[c])


def on_device(tokens, norm_gain, expert_ids, route_weights, gate_weight, up_weight, down_weight):
    tok_rows, half = tokens.shape
    experts = lax.axis_size("ep")
    side = math.isqrt(experts)
    top = expert_ids.shape[1]
    cap = max(2, (3 * tok_rows * top + 2 * experts - 1) // (2 * experts))
    width, part = gate_weight.shape[1:]
    S = side
    block = (cap // 8, 8, half)
    vmem = pl.BlockSpec(memory_space=pltpu.VMEM)
    hbm = pl.BlockSpec(memory_space=pltpu.HBM)
    dma = pltpu.SemaphoreType.DMA
    return pl.pallas_call(
        functools.partial(kernel, side, cap),
        out_shape=jax.ShapeDtypeStruct((tok_rows, half), BF16),
        in_specs=[hbm] + [vmem] * 3 + [hbm] * 3,
        out_specs=vmem,
        scratch_shapes=[
            pltpu.VMEM((tok_rows, half), BF16),
            pltpu.VMEM((2, width, part), BF16),
            pltpu.VMEM((2, width, part), BF16),
            pltpu.VMEM((2, 2 * part, half), BF16),
            pltpu.VMEM((S, S) + block, BF16),
            pltpu.VMEM((S, S) + block, BF16),
            pltpu.VMEM((S, S // 2, 2) + block, BF16),
            pltpu.VMEM((S, S // 2, 2) + block, BF16),
            pltpu.VMEM((S, S) + block, BF16),
            pltpu.VMEM((S, S) + block, BF16),
            pltpu.VMEM((S // 2 * cap, width), F32),
            pltpu.VMEM((tok_rows, half), F32),
            pltpu.VMEM((8, tok_rows), F32),
            pltpu.VMEM((tok_rows, 128), F32),
            dma((3,)), dma((3,)), dma((3,)), dma, pltpu.SemaphoreType.REGULAR,
            dma, dma, dma, dma,
            dma((S,)), dma((S,)), dma((S,)), dma((S,)), dma((S, 2)),
        ],
        compiler_params=pltpu.CompilerParams(
            collective_id=0, has_side_effects=True, vmem_limit_bytes=52 * 2**20
        ),
    )(tokens, norm_gain.reshape(1, -1), expert_ids.T, route_weights.T, gate_weight, up_weight, down_weight)


def solution(mesh):
    in_specs = (
        P(("grp", "ep"), "tp"),
        P(),
        P(("grp", "ep"), None),
        P(("grp", "ep"), None),
        P("ep", None, "tp"),
        P("ep", None, "tp"),
        P("ep", None, "tp"),
    )
    out_specs = P(("grp", "ep"), "tp")
    return jax.shard_map(
        on_device, mesh=mesh, in_specs=in_specs, out_specs=out_specs, check_vma=False
    )
```

```python
import functools
import math

import jax
import jax.numpy as jnp
from jax import lax
from jax.experimental import pallas as pl
from jax.experimental.pallas import tpu as pltpu
from jax.sharding import PartitionSpec as P

MESH = pl.DeviceIdType.MESH
BF16 = jnp.bfloat16
F32 = jnp.float32


def wrapped(v, side):
    v = jnp.where(v < 0, v + side, v)
    return jnp.where(v >= side, v - side, v)


def kernel(
    side, cap,
    tok_hbm, gain, ids, wts, gate_hbm, up_hbm, down_hbm, out,
    tok, wg, wu, wd, snd, rl1, rcv, res, rl2, back, normed, acc, posr, wts_hi_lo,
    s_w, r_w, l_w, l_t, go, known, s_a, s_b, s_c, s_d, r1, r2, r3, r3_last, r4,
):
    S = side
    half_side = S // 2
    c = lax.axis_index("tp")
    ep = lax.axis_index("ep")
    y = ep // S
    x = ep % S
    tok_rows = tok.shape[0]
    half = tok.shape[1]
    blocks = cap // 8

    def at(dx, dy):
        return ((y + dy + S) % S) * S + (x + dx + S) % S

    def send(src, dst, send_sem, recv_sem, chip, core):
        pltpu.make_async_remote_copy(
            src_ref=src, dst_ref=dst, send_sem=send_sem, recv_sem=recv_sem,
            device_id={"ep": chip, "tp": core}, device_id_type=MESH,
        ).start()

    def wait(sem, ref):
        pltpu.make_async_copy(ref, ref, sem).wait()

    tok_copy = pltpu.make_async_copy(tok_hbm, tok, l_t)
    tok_copy.start()

    barrier = pltpu.get_barrier_semaphore()

    @pl.when(c == 1)
    def _():
        for d in range(1, S):
            for h in range(2):
                pl.semaphore_signal(barrier, inc=1, device_id={"ep": at(d, 0), "tp": h}, device_id_type=MESH)
                pl.semaphore_signal(barrier, inc=1, device_id={"ep": at(0, d), "tp": h}, device_id_type=MESH)
        pl.semaphore_signal(barrier, inc=1, device_id={"ep": ep, "tp": 0}, device_id_type=MESH)

    weights = ((gate_hbm, wg), (up_hbm, wu), (down_hbm, wd))
    row = lax.broadcasted_iota(jnp.int32, (128, tok_rows), 0)
    e0 = ids[0:1, :]
    e1 = ids[1:2, :]
    hot0 = (row == e0).astype(F32)
    hot1 = (row == e1).astype(F32)
    earlier = (
        lax.broadcasted_iota(jnp.int32, (tok_rows, tok_rows), 0)
        < lax.broadcasted_iota(jnp.int32, (tok_rows, tok_rows), 1)
    )
    rank = jnp.dot(
        (hot0 + hot1).astype(BF16), earlier.astype(F32).astype(BF16), preferred_element_type=F32
    )
    pos0 = jnp.sum(rank * hot0, axis=0, keepdims=True) + (e0 * cap).astype(F32)
    pos1 = jnp.sum(rank * hot1, axis=0, keepdims=True) + (e1 * cap).astype(F32)
    posr[0:1, :] = pos0
    posr[1:2, :] = pos1

    def weight_table():
        w0 = wts[0:1, :]
        w1 = wts[1:2, :]
        w0_hi = w0.astype(BF16).astype(F32)
        w1_hi = w1.astype(BF16).astype(F32)
        row = lax.broadcasted_iota(jnp.int32, (128, tok_rows), 0)
        table = jnp.zeros((128, tok_rows), F32)
        columns = (posr[0:1, :], posr[1:2, :], w0_hi, w1_hi, w0 - w0_hi, w1 - w1_hi)
        for i, values in enumerate(columns):
            table = jnp.where(row == i, values, table)
        wts_hi_lo[...] = jnp.transpose(table)

    def first_axis(core, k):
        return (core + k) % 2

    def coords(j, k, core=c):
        f = first_axis(core, k)
        t = (j + (1 - 2 * f) * k + S) % S
        return t, j * (1 - f) + t * f, j * f + t * (1 - f)

    def positions(k, i, low, count):
        j = jnp.zeros(i.shape, jnp.int32)
        for m in range(1, count):
            j = j + (i >= m * cap).astype(jnp.int32)
        slot = i - j * cap
        j = j + low
        f = first_axis(c, k)
        t = wrapped(j + (1 - 2 * f) * k, S)
        dx = jnp.where(f == 0, j, t)
        dy = jnp.where(f == 0, t, j)
        e = wrapped(y + dy, S) * S + wrapped(x + dx, S)
        return (e * cap + slot).astype(F32)

    def gather(k):
        p = positions(k, lax.broadcasted_iota(jnp.int32, (S * cap, 1), 0), 0, S)
        pick = jnp.where(p == posr[0:1, :], 1.0, jnp.where(p == posr[1:2, :], 1.0, 0.0))
        rows = jnp.dot(pick.astype(BF16), tok[...], preferred_element_type=F32)
        snd[k] = rows.reshape(S, blocks, 8, half).astype(BF16)

    def dispatch(k, crossing):
        f = first_axis(c, k)
        for j in range(S):
            t, dx, dy = coords(j, k)
            p = dx % 2
            q = dx // 2
            now = (p == 0) if crossing else (p == 1)
            if j == 0:
                @pl.when(now & (t != 0))
                def _():
                    send(snd.at[k, j], rcv.at[k, q, c], s_a, r2.at[k], at(dx, dy), p)

                if crossing:
                    @pl.when((t == 0) & (c == 1))
                    def _():
                        send(snd.at[k, j], rcv.at[k, q, c], s_a, r2.at[k], ep, 0)
                else:
                    @pl.when((t == 0) & (c == 0))
                    def _():
                        rcv[0, 0, 0] = snd[0, 0]
            else:
                if not crossing:
                    @pl.when(t != 0)
                    def _():
                        send(snd.at[k, j], rl1.at[c, k, j], s_a, r1.at[c, k], at(j * (1 - f), j * f), 1)

                @pl.when(now & (t == 0))
                def _():
                    send(snd.at[k, j], rcv.at[k, q, c], s_a, r2.at[k], at(dx, dy), p)

    def dispatch_first(k):
        dispatch(k, False)

    def dispatch_crossing(k):
        dispatch(k, True)

    def wait_blocks(sem, ref, count):
        wait(sem, ref.at[pl.ds(0, count)])

    def wait_relayed(sem, ref, k):
        @pl.when(k == 0)
        def _():
            wait_blocks(sem, ref.at[k], S - 1)

        if S > 2:
            @pl.when(k != 0)
            def _():
                wait_blocks(sem, ref.at[k], S - 2)

    def relay_half(k, h):
        wait_relayed(r1.at[h, k], rl1.at[h], k)
        f = first_axis(h, k)
        for j in range(1, S):
            t, dx, dy = coords(j, k, h)

            @pl.when(t != 0)
            def _():
                send(rl1.at[h, k, j], rcv.at[k, dx // 2, h], s_b, r2.at[k], at(t * f, t * (1 - f)), dx % 2)

    def relay_dispatch(k):
        @pl.when(c == 1)
        def _():
            for h in range(2):
                relay_half(k, h)

    def send_relayed(k, j, src, chip, core):
        @pl.when(k == S - 1)
        def _():
            send(src, rl2.at[k, j], s_c, r3_last.at[j], chip, core)

        @pl.when(k != S - 1)
        def _():
            send(src, rl2.at[k, j], s_c, r3.at[k], chip, core)

    def expert(k):
        rows = cap
        own = (k == 0) & (c == 0)

        @pl.when(own)
        def _():
            wait_blocks(r2.at[k], back.at[k], S - 1)

        @pl.when(jnp.logical_not(own))
        def _():
            wait_blocks(r2.at[k], back.at[k], S)

        for q in range(S // 2):
            xa = rcv[k, q, 0].astype(F32).reshape(rows, half)
            xb = rcv[k, q, 1].astype(F32).reshape(rows, half)
            squares = jnp.sum(xa * xa, axis=1, keepdims=True) + jnp.sum(xb * xb, axis=1, keepdims=True)
            scale = lax.rsqrt(squares * (1.0 / (2 * half)) + 1e-06)
            normed[q * rows : (q + 1) * rows, :half] = xa * scale * gain[:, :half]
            normed[q * rows : (q + 1) * rows, half:] = xb * scale * gain[:, half:]
        xn = normed[...].astype(BF16)
        hidden = []
        for i in range(2):
            gate = jnp.dot(xn, wg[i], preferred_element_type=F32)
            upper = jnp.dot(xn, wu[i], preferred_element_type=F32)
            hidden.append((gate / (1.0 + jnp.exp(-gate)) * upper).astype(BF16))
        hidden = jnp.concatenate(hidden, axis=1)
        for h in range(2):
            result = jnp.dot(hidden, wd[h], preferred_element_type=F32)
            result = result.reshape(S // 2, blocks, 8, half).astype(BF16)
            for q in range(S // 2):
                res[k, q, h] = result[q]
        for q in range(S // 2):
            dx = 2 * q + c
            dy = (dx + k) % S
            direct = (dx == 0) | (dy == 0)
            for h in range(2):
                f = first_axis(h, k)
                j = dx * (1 - f) + dy * f

                @pl.when(jnp.logical_not(direct))
                def _():
                    send_relayed(k, j, res.at[k, q, h], at(-dx * (1 - f), -dy * f), h)

                away = direct if h else direct & ((dx != 0) | (dy != 0))

                @pl.when(away)
                def _():
                    send(res.at[k, q, h], back.at[k, j], s_c, r4.at[k, j // half_side], at(-dx, -dy), h)

                if q == 0 and h == 0:
                    @pl.when((k == 0) & (c == 0))
                    def _():
                        back[0, 0] = res[0, 0, 0]

    def relay_return(k):
        f = first_axis(c, k)

        @pl.when(k != S - 1)
        def _():
            wait_relayed(r3.at[k], rl2, k)

        for j in range(1, S):
            t, dx, dy = coords(j, k)

            @pl.when(t != 0)
            def _():
                @pl.when(k == S - 1)
                def _():
                    wait(r3_last.at[j], rl2.at[k, j])

                send(rl2.at[k, j], back.at[k, j], s_d, r4.at[k, j // half_side], at(-t * f, -t * (1 - f)), c)

    def combined(k, part):
        if part == 0:
            own = (k == 0) & (c == 0)

            @pl.when(own)
            def _():
                if half_side > 1:
                    wait_blocks(r4.at[k, part], back.at[k], half_side - 1)

            @pl.when(jnp.logical_not(own))
            def _():
                wait_blocks(r4.at[k, part], back.at[k], half_side)
        else:
            wait_blocks(r4.at[k, part], back.at[k], half_side)
        count = half_side * cap
        i = lax.broadcasted_iota(jnp.int32, (1, 2 * count), 1)
        high = i < count
        p = positions(k, jnp.where(high, i, i - count), part * half_side, half_side)
        one = jnp.where(high, wts_hi_lo[:, 2:3], wts_hi_lo[:, 4:5])
        two = jnp.where(high, wts_hi_lo[:, 3:4], wts_hi_lo[:, 5:6])
        mix = jnp.where(p == wts_hi_lo[:, 0:1], one, jnp.where(p == wts_hi_lo[:, 1:2], two, 0.0))
        rows = back[k, part * half_side : (part + 1) * half_side].astype(F32).reshape(count, half)
        rows = jnp.concatenate([rows, rows], axis=0).astype(BF16)
        return jnp.dot(mix.astype(BF16), rows, preferred_element_type=F32)

    def combine(k):
        for part in range(2):
            acc[...] += combined(k, part)

    def loop(low, high, *steps):
        def body(k, _):
            for step in steps:
                step(k)
            return 0

        lax.fori_loop(low, high, body, 0)

    tok_copy.wait()
    gather(0)
    pl.semaphore_wait(barrier, 2 * (S - 1) + 1 - c)

    @pl.when(c == 0)
    def _():
        pl.semaphore_signal(go, inc=1, device_id={"ep": ep, "tp": 1}, device_id_type=MESH)

    dispatch_first(0)
    loop(1, S, gather, dispatch_first)
    pl.semaphore_wait(go, 1)

    @pl.when(c == 1)
    def _():
        for d in range(1, S):
            pl.semaphore_signal(known, inc=1, device_id={"ep": at(d, 0), "tp": 1}, device_id_type=MESH)
            pl.semaphore_signal(known, inc=1, device_id={"ep": at(0, d), "tp": 1}, device_id_type=MESH)
        pl.semaphore_wait(known, 2 * (S - 1))
        pl.semaphore_signal(go, inc=1, device_id={"ep": ep, "tp": 0}, device_id_type=MESH)

    loop(0, S, dispatch_crossing)
    for i, (src, dst) in enumerate(weights):
        send(src.at[0], dst.at[c], s_w.at[i], r_w.at[i], ep, 1 - c)
        pltpu.make_async_copy(src.at[0], dst.at[c], l_w.at[i]).start()
    weight_table()
    acc[...] = jnp.zeros_like(acc)
    ahead = min(3, S)
    loop(0, ahead, relay_dispatch)
    for i, (src, dst) in enumerate(weights):
        wait(l_w.at[i], dst.at[c])
        wait(r_w.at[i], dst.at[1 - c])

    def relay_and_expert(k):
        @pl.when(k + ahead < S)
        def _():
            relay_dispatch(k + ahead)

        expert(k)

    loop(0, S, relay_and_expert)

    def relay_and_combine(k):
        @pl.when(k < S)
        def _():
            relay_return(k)

        @pl.when(k >= ahead)
        def _():
            combine(k - ahead)

    loop(0, S + ahead - 1, relay_and_combine)
    acc[...] += combined(S - 1, 0)
    out[...] = (acc[...] + combined(S - 1, 1)).astype(BF16)

    blocks_sent = S * S
    relayed = S - 1 + (S - 1) * (S - 2)

    def all_sent(sem, count):
        rows = count // S
        wait(sem, snd.at[pl.ds(0, rows)])
        if count % S:
            wait(sem, snd.at[0, pl.ds(0, count % S)])

    for sem in (s_a, s_c):
        @pl.when(c == 0)
        def _():
            all_sent(sem, blocks_sent - 1)

        @pl.when(c != 0)
        def _():
            all_sent(sem, blocks_sent)
    all_sent(s_d, relayed)

    @pl.when(c == 1)
    def _():
        for h in range(2):
            all_sent(s_b, relayed)

    for i, (src, dst) in enumerate(weights):
        wait(s_w.at[i], dst.at[c])


def on_device(tokens, norm_gain, expert_ids, route_weights, gate_weight, up_weight, down_weight):
    tok_rows, half = tokens.shape
    experts = lax.axis_size("ep")
    side = math.isqrt(experts)
    top = expert_ids.shape[1]
    cap = max(2, (3 * tok_rows * top + 2 * experts - 1) // (2 * experts))
    width, part = gate_weight.shape[1:]
    S = side
    block = (cap // 8, 8, half)
    vmem = pl.BlockSpec(memory_space=pltpu.VMEM)
    hbm = pl.BlockSpec(memory_space=pltpu.HBM)
    dma = pltpu.SemaphoreType.DMA
    return pl.pallas_call(
        functools.partial(kernel, side, cap),
        out_shape=jax.ShapeDtypeStruct((tok_rows, half), BF16),
        in_specs=[hbm] + [vmem] * 3 + [hbm] * 3,
        out_specs=vmem,
        scratch_shapes=[
            pltpu.VMEM((tok_rows, half), BF16),
            pltpu.VMEM((2, width, part), BF16),
            pltpu.VMEM((2, width, part), BF16),
            pltpu.VMEM((2, 2 * part, half), BF16),
            pltpu.VMEM((S, S) + block, BF16),
            pltpu.VMEM((2, S, S) + block, BF16),
            pltpu.VMEM((S, S // 2, 2) + block, BF16),
            pltpu.VMEM((S, S // 2, 2) + block, BF16),
            pltpu.VMEM((S, S) + block, BF16),
            pltpu.VMEM((S, S) + block, BF16),
            pltpu.VMEM((S // 2 * cap, width), F32),
            pltpu.VMEM((tok_rows, half), F32),
            pltpu.VMEM((8, tok_rows), F32),
            pltpu.VMEM((tok_rows, 128), F32),
            dma((3,)), dma((3,)), dma((3,)), dma, pltpu.SemaphoreType.REGULAR, pltpu.SemaphoreType.REGULAR,
            dma, dma, dma, dma,
            dma((2, S)), dma((S,)), dma((S,)), dma((S,)), dma((S, 2)),
        ],
        compiler_params=pltpu.CompilerParams(
            collective_id=0, has_side_effects=True, vmem_limit_bytes=52 * 2**20
        ),
    )(tokens, norm_gain.reshape(1, -1), expert_ids.T, route_weights.T, gate_weight, up_weight, down_weight)


def solution(mesh):
    in_specs = (
        P(("grp", "ep"), "tp"),
        P(),
        P(("grp", "ep"), None),
        P(("grp", "ep"), None),
        P("ep", None, "tp"),
        P("ep", None, "tp"),
        P("ep", None, "tp"),
    )
    out_specs = P(("grp", "ep"), "tp")
    return jax.shard_map(
        on_device, mesh=mesh, in_specs=in_specs, out_specs=out_specs, check_vma=False
    )
```

```python
import functools
import math

import jax
import jax.numpy as jnp
from jax import lax
from jax.experimental import pallas as pl
from jax.experimental.pallas import tpu as pltpu
from jax.sharding import PartitionSpec as P

MESH = pl.DeviceIdType.MESH
BF16 = jnp.bfloat16
F32 = jnp.float32


def wrapped(v, side):
    v = jnp.where(v < 0, v + side, v)
    return jnp.where(v >= side, v - side, v)


def kernel(
    side, cap,
    tok_hbm, gain, ids, wts, gate_hbm, up_hbm, down_hbm, out,
    tok, wg, wu, wd, snd, rl1, rcv, res, rl2, back, normed, acc, posr, wts_hi_lo,
    s_w, r_w, l_w, l_t, go, known, s_a, s_b, s_c, s_d, r1, r2, r3, r3_last, r4,
):
    S = side
    half_side = S // 2
    far_first = sorted(range(S), key=lambda j: -min(j, S - j))
    c = lax.axis_index("tp")
    ep = lax.axis_index("ep")
    y = ep // S
    x = ep % S
    tok_rows = tok.shape[0]
    half = tok.shape[1]
    blocks = cap // 8

    def at(dx, dy):
        return ((y + dy + S) % S) * S + (x + dx + S) % S

    def send(src, dst, send_sem, recv_sem, chip, core):
        pltpu.make_async_remote_copy(
            src_ref=src, dst_ref=dst, send_sem=send_sem, recv_sem=recv_sem,
            device_id={"ep": chip, "tp": core}, device_id_type=MESH,
        ).start()

    def wait(sem, ref):
        pltpu.make_async_copy(ref, ref, sem).wait()

    tok_copy = pltpu.make_async_copy(tok_hbm, tok, l_t)
    tok_copy.start()

    barrier = pltpu.get_barrier_semaphore()

    @pl.when(c == 1)
    def _():
        for d in range(1, S):
            for h in range(2):
                pl.semaphore_signal(barrier, inc=1, device_id={"ep": at(d, 0), "tp": h}, device_id_type=MESH)
                pl.semaphore_signal(barrier, inc=1, device_id={"ep": at(0, d), "tp": h}, device_id_type=MESH)
        pl.semaphore_signal(barrier, inc=1, device_id={"ep": ep, "tp": 0}, device_id_type=MESH)

    weights = ((gate_hbm, wg), (up_hbm, wu), (down_hbm, wd))
    row = lax.broadcasted_iota(jnp.int32, (128, tok_rows), 0)
    e0 = ids[0:1, :]
    e1 = ids[1:2, :]
    hot0 = (row == e0).astype(F32)
    hot1 = (row == e1).astype(F32)
    earlier = (
        lax.broadcasted_iota(jnp.int32, (tok_rows, tok_rows), 0)
        < lax.broadcasted_iota(jnp.int32, (tok_rows, tok_rows), 1)
    )
    rank = jnp.dot(
        (hot0 + hot1).astype(BF16), earlier.astype(F32).astype(BF16), preferred_element_type=F32
    )
    pos0 = jnp.sum(rank * hot0, axis=0, keepdims=True) + (e0 * cap).astype(F32)
    pos1 = jnp.sum(rank * hot1, axis=0, keepdims=True) + (e1 * cap).astype(F32)
    posr[0:1, :] = pos0
    posr[1:2, :] = pos1

    def weight_table():
        w0 = wts[0:1, :]
        w1 = wts[1:2, :]
        w0_hi = w0.astype(BF16).astype(F32)
        w1_hi = w1.astype(BF16).astype(F32)
        row = lax.broadcasted_iota(jnp.int32, (128, tok_rows), 0)
        table = jnp.zeros((128, tok_rows), F32)
        columns = (posr[0:1, :], posr[1:2, :], w0_hi, w1_hi, w0 - w0_hi, w1 - w1_hi)
        for i, values in enumerate(columns):
            table = jnp.where(row == i, values, table)
        wts_hi_lo[...] = jnp.transpose(table)

    def first_axis(core, k):
        return (core + k) % 2

    def coords(j, k, core=c):
        f = first_axis(core, k)
        t = (j + (1 - 2 * f) * k + S) % S
        return t, j * (1 - f) + t * f, j * f + t * (1 - f)

    def positions(k, i, low, count):
        j = jnp.zeros(i.shape, jnp.int32)
        for m in range(1, count):
            j = j + (i >= m * cap).astype(jnp.int32)
        slot = i - j * cap
        j = j + low
        f = first_axis(c, k)
        t = wrapped(j + (1 - 2 * f) * k, S)
        dx = jnp.where(f == 0, j, t)
        dy = jnp.where(f == 0, t, j)
        e = wrapped(y + dy, S) * S + wrapped(x + dx, S)
        return (e * cap + slot).astype(F32)

    def gather(k):
        p = positions(k, lax.broadcasted_iota(jnp.int32, (S * cap, 1), 0), 0, S)
        pick = jnp.where(p == posr[0:1, :], 1.0, jnp.where(p == posr[1:2, :], 1.0, 0.0))
        rows = jnp.dot(pick.astype(BF16), tok[...], preferred_element_type=F32)
        snd[k] = rows.reshape(S, blocks, 8, half).astype(BF16)

    def dispatch(k, crossing):
        f = first_axis(c, k)
        for j in far_first:
            t, dx, dy = coords(j, k)
            p = dx % 2
            q = dx // 2
            now = (p == 0) if crossing else (p == 1)
            if j == 0:
                @pl.when(now & (t != 0))
                def _():
                    send(snd.at[k, j], rcv.at[k, q, c], s_a, r2.at[k], at(dx, dy), p)

                if crossing:
                    @pl.when((t == 0) & (c == 1))
                    def _():
                        send(snd.at[k, j], rcv.at[k, q, c], s_a, r2.at[k], ep, 0)
                else:
                    @pl.when((t == 0) & (c == 0))
                    def _():
                        rcv[0, 0, 0] = snd[0, 0]
            else:
                if not crossing:
                    @pl.when(t != 0)
                    def _():
                        send(snd.at[k, j], rl1.at[c, k, j], s_a, r1.at[c, k], at(j * (1 - f), j * f), 1)

                @pl.when(now & (t == 0))
                def _():
                    send(snd.at[k, j], rcv.at[k, q, c], s_a, r2.at[k], at(dx, dy), p)

    def dispatch_first(k):
        dispatch(k, False)

    def dispatch_crossing(k):
        dispatch(k, True)

    def wait_blocks(sem, ref, count):
        wait(sem, ref.at[pl.ds(0, count)])

    def wait_relayed(sem, ref, k):
        @pl.when(k == 0)
        def _():
            wait_blocks(sem, ref.at[k], S - 1)

        if S > 2:
            @pl.when(k != 0)
            def _():
                wait_blocks(sem, ref.at[k], S - 2)

    def relay_half(k, h):
        wait_relayed(r1.at[h, k], rl1.at[h], k)
        f = first_axis(h, k)
        for j in far_first[:-1]:
            t, dx, dy = coords(j, k, h)

            @pl.when(t != 0)
            def _():
                send(rl1.at[h, k, j], rcv.at[k, dx // 2, h], s_b, r2.at[k], at(t * f, t * (1 - f)), dx % 2)

    def relay_dispatch(k):
        @pl.when(c == 1)
        def _():
            for h in range(2):
                relay_half(k, h)

    def send_relayed(k, j, src, chip, core):
        @pl.when(k == S - 1)
        def _():
            send(src, rl2.at[k, j], s_c, r3_last.at[j], chip, core)

        @pl.when(k != S - 1)
        def _():
            send(src, rl2.at[k, j], s_c, r3.at[k], chip, core)

    def expert(k):
        rows = cap
        own = (k == 0) & (c == 0)

        @pl.when(own)
        def _():
            wait_blocks(r2.at[k], back.at[k], S - 1)

        @pl.when(jnp.logical_not(own))
        def _():
            wait_blocks(r2.at[k], back.at[k], S)

        for q in range(S // 2):
            xa = rcv[k, q, 0].astype(F32).reshape(rows, half)
            xb = rcv[k, q, 1].astype(F32).reshape(rows, half)
            squares = jnp.sum(xa * xa, axis=1, keepdims=True) + jnp.sum(xb * xb, axis=1, keepdims=True)
            scale = lax.rsqrt(squares * (1.0 / (2 * half)) + 1e-06)
            normed[q * rows : (q + 1) * rows, :half] = xa * scale * gain[:, :half]
            normed[q * rows : (q + 1) * rows, half:] = xb * scale * gain[:, half:]
        xn = normed[...].astype(BF16)
        hidden = []
        for i in range(2):
            gate = jnp.dot(xn, wg[i], preferred_element_type=F32)
            upper = jnp.dot(xn, wu[i], preferred_element_type=F32)
            hidden.append((gate / (1.0 + jnp.exp(-gate)) * upper).astype(BF16))
        hidden = jnp.concatenate(hidden, axis=1)
        for h in range(2):
            result = jnp.dot(hidden, wd[h], preferred_element_type=F32)
            result = result.reshape(S // 2, blocks, 8, half).astype(BF16)
            for q in range(S // 2):
                res[k, q, h] = result[q]
        for q in range(S // 2):
            dx = 2 * q + c
            dy = (dx + k) % S
            direct = (dx == 0) | (dy == 0)
            for h in range(2):
                f = first_axis(h, k)
                j = dx * (1 - f) + dy * f

                @pl.when(jnp.logical_not(direct))
                def _():
                    send_relayed(k, j, res.at[k, q, h], at(-dx * (1 - f), -dy * f), h)

                away = direct if h else direct & ((dx != 0) | (dy != 0))

                @pl.when(away)
                def _():
                    send(res.at[k, q, h], back.at[k, j], s_c, r4.at[k, j // half_side], at(-dx, -dy), h)

                if q == 0 and h == 0:
                    @pl.when((k == 0) & (c == 0))
                    def _():
                        back[0, 0] = res[0, 0, 0]

    def relay_return(k):
        f = first_axis(c, k)

        @pl.when(k != S - 1)
        def _():
            wait_relayed(r3.at[k], rl2, k)

        for j in range(1, S):
            t, dx, dy = coords(j, k)

            @pl.when(t != 0)
            def _():
                @pl.when(k == S - 1)
                def _():
                    wait(r3_last.at[j], rl2.at[k, j])

                send(rl2.at[k, j], back.at[k, j], s_d, r4.at[k, j // half_side], at(-t * f, -t * (1 - f)), c)

    def combined(k, part):
        if part == 0:
            own = (k == 0) & (c == 0)

            @pl.when(own)
            def _():
                if half_side > 1:
                    wait_blocks(r4.at[k, part], back.at[k], half_side - 1)

            @pl.when(jnp.logical_not(own))
            def _():
                wait_blocks(r4.at[k, part], back.at[k], half_side)
        else:
            wait_blocks(r4.at[k, part], back.at[k], half_side)
        count = half_side * cap
        i = lax.broadcasted_iota(jnp.int32, (1, 2 * count), 1)
        high = i < count
        p = positions(k, jnp.where(high, i, i - count), part * half_side, half_side)
        one = jnp.where(high, wts_hi_lo[:, 2:3], wts_hi_lo[:, 4:5])
        two = jnp.where(high, wts_hi_lo[:, 3:4], wts_hi_lo[:, 5:6])
        mix = jnp.where(p == wts_hi_lo[:, 0:1], one, jnp.where(p == wts_hi_lo[:, 1:2], two, 0.0))
        rows = back[k, part * half_side : (part + 1) * half_side].astype(F32).reshape(count, half)
        rows = jnp.concatenate([rows, rows], axis=0).astype(BF16)
        return jnp.dot(mix.astype(BF16), rows, preferred_element_type=F32)

    def combine(k):
        for part in range(2):
            acc[...] += combined(k, part)

    def loop(low, high, *steps):
        def body(k, _):
            for step in steps:
                step(k)
            return 0

        lax.fori_loop(low, high, body, 0)

    tok_copy.wait()
    gather(0)
    pl.semaphore_wait(barrier, 2 * (S - 1) + 1 - c)

    @pl.when(c == 0)
    def _():
        pl.semaphore_signal(go, inc=1, device_id={"ep": ep, "tp": 1}, device_id_type=MESH)

    dispatch_first(0)
    loop(1, S, gather, dispatch_first)
    pl.semaphore_wait(go, 1)

    @pl.when(c == 1)
    def _():
        for d in range(1, S):
            pl.semaphore_signal(known, inc=1, device_id={"ep": at(d, 0), "tp": 1}, device_id_type=MESH)
            pl.semaphore_signal(known, inc=1, device_id={"ep": at(0, d), "tp": 1}, device_id_type=MESH)
        pl.semaphore_wait(known, 2 * (S - 1))
        pl.semaphore_signal(go, inc=1, device_id={"ep": ep, "tp": 0}, device_id_type=MESH)

    loop(0, S, dispatch_crossing)
    for i, (src, dst) in enumerate(weights):
        send(src.at[0], dst.at[c], s_w.at[i], r_w.at[i], ep, 1 - c)
        pltpu.make_async_copy(src.at[0], dst.at[c], l_w.at[i]).start()
    weight_table()
    acc[...] = jnp.zeros_like(acc)
    ahead = min(3, S)
    loop(0, ahead, relay_dispatch)
    for i, (src, dst) in enumerate(weights):
        wait(l_w.at[i], dst.at[c])
        wait(r_w.at[i], dst.at[1 - c])

    def relay_and_expert(k):
        @pl.when(k + ahead < S)
        def _():
            relay_dispatch(k + ahead)

        expert(k)

    loop(0, S, relay_and_expert)

    def relay_and_combine(k):
        @pl.when(k < S)
        def _():
            relay_return(k)

        @pl.when(k >= ahead)
        def _():
            combine(k - ahead)

    loop(0, S + ahead - 1, relay_and_combine)
    acc[...] += combined(S - 1, 0)
    out[...] = (acc[...] + combined(S - 1, 1)).astype(BF16)

    blocks_sent = S * S
    relayed = S - 1 + (S - 1) * (S - 2)

    def all_sent(sem, count):
        rows = count // S
        wait(sem, snd.at[pl.ds(0, rows)])
        if count % S:
            wait(sem, snd.at[0, pl.ds(0, count % S)])

    for sem in (s_a, s_c):
        @pl.when(c == 0)
        def _():
            all_sent(sem, blocks_sent - 1)

        @pl.when(c != 0)
        def _():
            all_sent(sem, blocks_sent)
    all_sent(s_d, relayed)

    @pl.when(c == 1)
    def _():
        for h in range(2):
            all_sent(s_b, relayed)

    for i, (src, dst) in enumerate(weights):
        wait(s_w.at[i], dst.at[c])


def on_device(tokens, norm_gain, expert_ids, route_weights, gate_weight, up_weight, down_weight):
    tok_rows, half = tokens.shape
    experts = lax.axis_size("ep")
    side = math.isqrt(experts)
    top = expert_ids.shape[1]
    cap = max(2, (3 * tok_rows * top + 2 * experts - 1) // (2 * experts))
    width, part = gate_weight.shape[1:]
    S = side
    block = (cap // 8, 8, half)
    vmem = pl.BlockSpec(memory_space=pltpu.VMEM)
    hbm = pl.BlockSpec(memory_space=pltpu.HBM)
    dma = pltpu.SemaphoreType.DMA
    return pl.pallas_call(
        functools.partial(kernel, side, cap),
        out_shape=jax.ShapeDtypeStruct((tok_rows, half), BF16),
        in_specs=[hbm] + [vmem] * 3 + [hbm] * 3,
        out_specs=vmem,
        scratch_shapes=[
            pltpu.VMEM((tok_rows, half), BF16),
            pltpu.VMEM((2, width, part), BF16),
            pltpu.VMEM((2, width, part), BF16),
            pltpu.VMEM((2, 2 * part, half), BF16),
            pltpu.VMEM((S, S) + block, BF16),
            pltpu.VMEM((2, S, S) + block, BF16),
            pltpu.VMEM((S, S // 2, 2) + block, BF16),
            pltpu.VMEM((S, S // 2, 2) + block, BF16),
            pltpu.VMEM((S, S) + block, BF16),
            pltpu.VMEM((S, S) + block, BF16),
            pltpu.VMEM((S // 2 * cap, width), F32),
            pltpu.VMEM((tok_rows, half), F32),
            pltpu.VMEM((8, tok_rows), F32),
            pltpu.VMEM((tok_rows, 128), F32),
            dma((3,)), dma((3,)), dma((3,)), dma, pltpu.SemaphoreType.REGULAR, pltpu.SemaphoreType.REGULAR,
            dma, dma, dma, dma,
            dma((2, S)), dma((S,)), dma((S,)), dma((S,)), dma((S, 2)),
        ],
        compiler_params=pltpu.CompilerParams(
            collective_id=0, has_side_effects=True, vmem_limit_bytes=52 * 2**20
        ),
    )(tokens, norm_gain.reshape(1, -1), expert_ids.T, route_weights.T, gate_weight, up_weight, down_weight)


def solution(mesh):
    in_specs = (
        P(("grp", "ep"), "tp"),
        P(),
        P(("grp", "ep"), None),
        P(("grp", "ep"), None),
        P("ep", None, "tp"),
        P("ep", None, "tp"),
        P("ep", None, "tp"),
    )
    out_specs = P(("grp", "ep"), "tp")
    return jax.shard_map(
        on_device, mesh=mesh, in_specs=in_specs, out_specs=out_specs, check_vma=False
    )
```
